32 devices in a mesh: sp: 16 (over z, y, core), tp: 2 (over x).
Axes of the slice: x: 2, y: 2, z: 4, core: 2. Of those that a mesh axis runs over, the one named last changes fastest.
Arguments:
- query_rows: bfloat16 [8192, 1024], P(('sp', 'tp')), may hold values from -6 to 6
- key_rows: bfloat16 [8192, 1024], P(('sp', 'tp')), may hold values from -6 to 6
- value_rows: bfloat16 [8192, 1024], P(('sp', 'tp')), may hold values from -6 to 6
- out_grad: bfloat16 [8192, 1024], P(('sp', 'tp')), may hold values from -40 to 40
- log_totals: float32 [8192, 8], P(('sp', 'tp')), may hold values from 6 to 7.5
- out_dot: float32 [8192, 8], P(('sp', 'tp')), may hold values from -6 to 6
- bias_table: float32 [8, 320], replicated, may hold values from -4 to 4
Outputs:
- grad_query: bfloat16 [8192, 1024], P(('sp', 'tp'))
- grad_key: bfloat16 [8192, 1024], P(('sp', 'tp'))
- grad_value: bfloat16 [8192, 1024], P(('sp', 'tp'))
- grad_table: float32 [8, 320], replicated
The draws below stay inside these ranges and needn't reach their ends.
All inputs are finite; a program needn't handle non-finite values.
Results may differ from the reference program's by a relative error of at most 0.005.
Values may be sent and summed in bfloat16 or wider, within the bound.
No kernel may reach another device: no remote copies, remote signals or barrier semaphores. Data moves between devices by JAX's collectives and lax.ppermute only.
A program may use at most 128 MiB of HBM per device.

```python
import jax
import jax.numpy as jnp
from jax import lax

HEADS = 8
HEAD_DIM = 128
SEG_LEN = 64
LEFT_SEGS = 8
REL_CLIP = 256
TOK_DEV = 256
MIX_WIDTH = 1024
TABLE_LEN = 320
BACK_DEVS = 2
TOKENS = 8192


def draw_out_grad(key, part):
    position = jnp.arange(TOKENS, dtype=jnp.float32) / TOKENS
    base_vals = jnp.clip(jax.random.normal(key, (TOKENS, HEADS * HEAD_DIM), jnp.float32), -6.0, 6.0)
    growth = 3.0 ** position
    return (base_vals * growth[:, None]).astype(jnp.bfloat16)


def block_levels(rng, shape, shards, low, largest):
    loudness, own = 1.0, jax.random.fold_in(rng, 6)
    for axis_at, shards_of in shards:
        heights = jnp.exp(jax.random.uniform(jax.random.fold_in(own, axis_at), (shards_of,), jnp.float32, low / len(shards), largest / len(shards)))
        loudness = loudness * jnp.repeat(heights, shape[axis_at] // shards_of).reshape([-1 if axis == axis_at else 1 for axis in range(len(shape))])
    return loudness


def noise(key, shape, deviation, bound, cuts=(), held_as=jnp.bfloat16):
    entries = jax.random.normal(key, shape, jnp.float32) * deviation
    if len(cuts) > 0:
        entries = block_levels(key, shape, cuts, -0.22, 0.18) * entries
    return jnp.clip(entries, min=-bound, max=bound).astype(held_as)


def setup_inputs(seed: int = 0) -> dict:
    key_of = jax.random.split(jax.random.key(seed), 8)
    query_rows = noise(key_of[0], (TOKENS, MIX_WIDTH), 1.0, 6.0, ((0, 32),))
    key_rows = noise(key_of[1], (TOKENS, MIX_WIDTH), 1.0, 6.0, ((0, 32),))
    value_rows = noise(key_of[2], (TOKENS, MIX_WIDTH), 1.0, 6.0, ((0, 32),))
    out_grad = draw_out_grad(jax.random.fold_in(key_of[7], 71), 0)
    log_totals = jnp.clip(6.0 + 1.5 * jax.random.uniform(key_of[4], (TOKENS, HEADS), jnp.float32) ** block_levels(key_of[4], (TOKENS, HEADS), ((0, 32),), -0.2, 0.2), 6.0, 7.5)
    out_dot = noise(key_of[5], (TOKENS, HEADS), 1.5, 6.0, ((0, 32),), jnp.float32)
    bias_table = noise(key_of[6], (HEADS, TABLE_LEN), 1.0, 4.0, (), jnp.float32)
    return dict(query_rows=query_rows, key_rows=key_rows, value_rows=value_rows, out_grad=out_grad, log_totals=log_totals, out_dot=out_dot, bias_table=bias_table)


def reference(query_rows, key_rows, value_rows, out_grad, log_totals, out_dot, bias_table):
    token_count = query_rows.shape[0]
    feature_count = query_rows.shape[1]
    head_count = bias_table.shape[0]
    head_size = feature_count // head_count
    block_rows = TOK_DEV
    lag_rows = BACK_DEVS * TOK_DEV
    window = lag_rows + block_rows
    inv_root = head_size ** -0.5
    padded_keys = jnp.concatenate([jnp.zeros((lag_rows, feature_count), query_rows.dtype), key_rows], axis=0)
    padded_values = jnp.concatenate([jnp.zeros((lag_rows, feature_count), query_rows.dtype), value_rows], axis=0)
    local_query = jnp.arange(block_rows, dtype=jnp.int32)
    local_key = jnp.arange(window, dtype=jnp.int32)
    distance = local_query[:, None] - local_key[None, :] + lag_rows
    table_index = (jnp.clip(distance, 1 - SEG_LEN, REL_CLIP) + SEG_LEN - 1).astype(jnp.int32)
    bias_vals = bias_table[:, table_index]
    seg_gap = (local_query[:, None] + lag_rows) // SEG_LEN - (local_key // SEG_LEN)[None, :]
    band_ok = (seg_gap >= 0) & (seg_gap <= LEFT_SEGS)

    def one_block(totals, block_id):
        key_grads, value_grads, table_grad = totals
        first_row = (block_id * block_rows).astype(jnp.int32)
        queries = lax.dynamic_slice_in_dim(query_rows, first_row, block_rows, 0).astype(jnp.float32)
        queries = queries.reshape(block_rows, head_count, head_size)
        grads_out = lax.dynamic_slice_in_dim(out_grad, first_row, block_rows, 0).astype(jnp.float32)
        grads_out = grads_out.reshape(block_rows, head_count, head_size)
        log_rows = lax.dynamic_slice_in_dim(log_totals, first_row, block_rows, 0)
        dot_rows = lax.dynamic_slice_in_dim(out_dot, first_row, block_rows, 0)
        keys = lax.dynamic_slice_in_dim(padded_keys, first_row, window, 0).astype(jnp.float32)
        keys = keys.reshape(window, head_count, head_size)
        values = lax.dynamic_slice_in_dim(padded_values, first_row, window, 0).astype(jnp.float32)
        values = values.reshape(window, head_count, head_size)
        allowed = band_ok & ((first_row - lag_rows + local_key) >= 0)[None, :]
        scores = jnp.einsum('phd,rhd->hpr', queries, keys) * inv_root + bias_vals
        weights = jnp.where(allowed[None], jnp.exp(scores - log_rows.T[:, :, None]), 0.0)
        weights_b = lax.optimization_barrier(weights.astype(jnp.bfloat16)).astype(jnp.float32)
        weight_grads = jnp.einsum('phd,rhd->hpr', grads_out, values)
        score_grads = weights * (weight_grads - dot_rows.T[:, :, None])
        score_grads_b = lax.optimization_barrier(score_grads.astype(jnp.bfloat16)).astype(jnp.float32)
        block_query = jnp.einsum('hpr,rhd->phd', score_grads_b, keys) * inv_root
        block_key = (jnp.einsum('hpr,phd->rhd', score_grads_b, queries) * inv_root).reshape(window, feature_count)
        block_value = jnp.einsum('hpr,phd->rhd', weights_b, grads_out).reshape(window, feature_count)
        table_part = jax.ops.segment_sum(score_grads.reshape(head_count, -1).T, table_index.reshape(-1),
                                         num_segments=TABLE_LEN).T
        key_grads = lax.dynamic_update_slice_in_dim(
            key_grads, lax.dynamic_slice_in_dim(key_grads, first_row, window, 0) + block_key, first_row, 0)
        value_grads = lax.dynamic_update_slice_in_dim(
            value_grads, lax.dynamic_slice_in_dim(value_grads, first_row, window, 0) + block_value, first_row, 0)
        result_rows = block_query.reshape(block_rows, feature_count).astype(jnp.bfloat16)
        return (key_grads, value_grads, table_grad + table_part), result_rows

    start_totals = (jnp.zeros((lag_rows + token_count, feature_count), jnp.float32),
                    jnp.zeros((lag_rows + token_count, feature_count), jnp.float32),
                    jnp.zeros((head_count, TABLE_LEN), jnp.float32))
    block_ids = jnp.arange(token_count // block_rows, dtype=jnp.int32)
    (key_grads, value_grads, table_grad), query_grads = lax.scan(one_block, start_totals, block_ids)
    grad_query = query_grads.reshape(token_count, feature_count)
    grad_key = key_grads[lag_rows:].astype(jnp.bfloat16)
    grad_value = value_grads[lag_rows:].astype(jnp.bfloat16)
    return (grad_query, grad_key, grad_value, table_grad)
```

```python
import functools
import math

import jax
import jax.numpy as jnp
from jax import lax
from jax.experimental import pallas as pl
from jax.experimental.pallas import tpu as pltpu
from jax.sharding import PartitionSpec as P

SEG_LEN = 64
LEFT_SEGS = 8
REL_CLIP = 256
AXES = ("sp", "tp")
LOG2E = math.log2(math.e)
MASKED = -1e30
F32 = jnp.float32
BF16 = jnp.bfloat16
NT = (((1,), (1,)), ((), ()))
NN = (((1,), (0,)), ((), ()))
TN = (((0,), (0,)), ((), ()))


def shifted(block, distance):
    count = lax.axis_size(AXES)
    route = [(i - distance, i) for i in range(count) if 0 <= i - distance < count]
    return lax.ppermute(block, AXES, route)


def prime_radices(count):
    radices = []
    twos = 0
    while count % 2 == 0:
        count //= 2
        twos += 1
    while twos > 0:
        take = 2 if twos != 3 else 3
        take = min(take, twos)
        radices.append(2**take)
        twos -= take
    factor = 3
    while count > 1:
        while count % factor == 0:
            radices.append(factor)
            count //= factor
        factor += 2
    return radices


def pair_tree(parts):
    while len(parts) > 1:
        parts = [parts[i] + parts[i + 1] for i in range(0, len(parts), 2)]
    return parts[0]


def all_sum(part):
    count = lax.axis_size(AXES)
    me = lax.axis_index(AXES)
    stride = 1
    for radix in prime_radices(count):
        if radix & (radix - 1) == 0:
            parts = [part]
            for step in range(1, radix):
                route = [(i, i ^ (step * stride)) for i in range(count)]
                parts.append(lax.ppermute(part, AXES, route))
            part = pair_tree(parts)
        else:
            digit = (me // stride) % radix
            parts = [part]
            for step in range(1, radix):
                route = []
                for i in range(count):
                    d = (i // stride) % radix
                    route.append((i, i + (((d - step) % radix) - d) * stride))
                parts.append(lax.ppermute(part, AXES, route))
            total = jnp.zeros_like(part)
            for d in range(radix):
                value = parts[0]
                for step in range(1, radix):
                    value = jnp.where((digit + step) % radix == d, parts[step], value)
                total = total + value
            part = total
        stride *= radix
    return part


def bias_kernel(chunk_ref, tile_ref):
    size = chunk_ref.shape[2]
    row = lax.broadcasted_iota(jnp.int32, (size, size), 0)
    col = lax.broadcasted_iota(jnp.int32, (size, size), 1)
    rolled = []
    for c in range(4):
        line = jnp.broadcast_to(chunk_ref[0, c : c + 1, :] * LOG2E, (size, size))
        rolled.append(pltpu.roll(line, 0, 1, stride=1, stride_axis=0))
    for b in range(3):
        tile = jnp.where(col >= row, rolled[b + 1], rolled[b])
        if b == 0:
            tile = jnp.where((row // SEG_LEN) <= (col // SEG_LEN), tile, MASKED)
        tile_ref[0, b] = tile


def unroll_sum(tile):
    size = tile.shape[0]
    group = 8
    parts = []
    for start in range(0, size, group):
        part = tile[start : start + group, :]
        parts.append(part if start == 0 else pltpu.roll(part, size - start, 1))
    total = pair_tree(parts)
    row = lax.broadcasted_iota(jnp.int32, total.shape, 0)
    for bit in (1, 2, 4):
        total = jnp.where((row & bit) != 0, pltpu.roll(total, size - bit, 1), total)
    return jnp.sum(total, axis=0, keepdims=True)


def score_terms(lag, key, value, query, grad, log_row, dot_row, tiles, const, inv_root):
    rows = key.shape[0]
    half = rows // 2
    raw = lax.dot_general(key, query, NT, preferred_element_type=F32)
    wgt = lax.dot_general(value, grad, NT, preferred_element_type=F32)
    row = lax.broadcasted_iota(jnp.int32, (half, half), 0) // SEG_LEN
    col = lax.broadcasted_iota(jnp.int32, (half, half), 1) // SEG_LEN
    acc = [None, None, None, None]
    w_rows, s_rows = [], []
    for r in range(2):
        w_cols, s_cols = [], []
        for c in range(2):
            if (lag == 0 and r > c) or (lag == 2 and c > r):
                w_cols.append(jnp.zeros((half, half), BF16))
                s_cols.append(jnp.zeros((half, half), BF16))
                continue
            rs, cs = slice(r * half, (r + 1) * half), slice(c * half, (c + 1) * half)
            level = min(2 * lag + c - r, 3)
            lrow = log_row[:, cs]
            bias = const - lrow if level == 3 else tiles[level] - lrow
            weight = jnp.exp2(raw[rs, cs] * (inv_root * LOG2E) + bias)
            if lag == 2 and r == c:
                weight = jnp.where(col <= row, weight, 0.0)
            score = weight * (wgt[rs, cs] - dot_row[:, cs])
            acc[level] = score if acc[level] is None else acc[level] + score
            w_cols.append(weight.astype(BF16))
            s_cols.append(score.astype(BF16))
        w_rows.append(jnp.concatenate(w_cols, axis=1))
        s_rows.append(jnp.concatenate(s_cols, axis=1))
    return jnp.concatenate(w_rows, axis=0), jnp.concatenate(s_rows, axis=0), acc


def table_lines(acc, size):
    row = lax.broadcasted_iota(jnp.int32, (size, size), 0)
    col = lax.broadcasted_iota(jnp.int32, (size, size), 1)
    lines = []
    for c in range(4):
        upper = acc[c - 1] if c > 0 else None
        lower = acc[c] if c < 3 else None
        line = None
        if upper is not None or lower is not None:
            zero = jnp.zeros((size, size), F32)
            mixed = jnp.where(
                col >= row,
                zero if upper is None else upper,
                zero if lower is None else lower,
            )
            line = unroll_sum(mixed)
        if c == 3 and acc[3] is not None:
            extra = jnp.sum(acc[3], axis=0, keepdims=True)
            line = extra if line is None else line + extra
        lines.append(jnp.zeros((1, size), F32) if line is None else line)
    return jnp.concatenate(lines, axis=0)


def lag_kernel(lag, heads_step, head_count, split, *refs):
    if lag == 0:
        (k_ref, v_ref, q_ref, g_ref, st_ref, tile_ref, chunk_ref, dq_ref, dk_ref, dv_ref, tab_ref) = refs
    elif not split:
        (k_ref, v_ref, q_ref, g_ref, st_ref, tile_ref, chunk_ref, dk_in, dv_in, tab_in,
         dq_ref, dk_ref, dv_ref, tab_ref) = refs
    else:
        (k_ref, v_ref, q_ref, g_ref, st_ref, tile_ref, chunk_ref, tab_in,
         dq_ref, tab_ref, w_ref, s_ref) = refs
    size = chunk_ref.shape[2]
    head_dim = k_ref.shape[1] // heads_step
    inv_root = head_dim ** (-0.5)
    step = pl.program_id(0)
    for i in range(heads_step):
        head = step * heads_step + i
        cols = slice(i * head_dim, (i + 1) * head_dim)
        key, value, query, grad = k_ref[:, cols], v_ref[:, cols], q_ref[:, cols], g_ref[:, cols]
        log_row = st_ref[pl.ds(head, 1), :]
        dot_row = st_ref[pl.ds(head + head_count, 1), :]
        const = chunk_ref[i, 3:4, :] * LOG2E
        tiles = [None if lag == 2 else tile_ref[i, b] for b in range(3)]
        weights, scores, acc = score_terms(
            lag, key, value, query, grad, log_row, dot_row, tiles, const, inv_root
        )
        dq = lax.dot_general(scores, key, TN, preferred_element_type=F32) * inv_root
        dq_ref[:, cols] = dq.astype(dq_ref.dtype)
        lines = table_lines(acc, size)
        tab_ref[i] = lines if lag == 0 else lines + tab_in[i]
        if split:
            w_ref[i] = weights
            s_ref[i] = scores
        else:
            dk = lax.dot_general(scores, query, NN, preferred_element_type=F32)
            dv = lax.dot_general(weights, grad, NN, preferred_element_type=F32)
            dk_ref[:, cols] = dk if lag == 0 else dk + dk_in[:, cols]
            dv_ref[:, cols] = dv if lag == 0 else dv + dv_in[:, cols]


def close_kernel(heads_step, w_ref, s_ref, q_ref, g_ref, dk_in, dv_in, dk_ref, dv_ref):
    head_dim = q_ref.shape[1] // heads_step
    inv_root = head_dim ** (-0.5)
    for i in range(heads_step):
        cols = slice(i * head_dim, (i + 1) * head_dim)
        dk = lax.dot_general(s_ref[i], q_ref[:, cols], NN, preferred_element_type=F32)
        dv = lax.dot_general(w_ref[i], g_ref[:, cols], NN, preferred_element_type=F32)
        dk_ref[:, cols] = ((dk + dk_in[:, cols]) * inv_root).astype(BF16)
        dv_ref[:, cols] = (dv + dv_in[:, cols]).astype(BF16)


def local(query_rows, key_rows, value_rows, out_grad, log_totals, out_dot, bias_table):
    rows, feats = query_rows.shape
    heads = log_totals.shape[1]
    table_len = bias_table.shape[1]
    half = rows // 2
    heads_step = 2
    grid = (heads // heads_step,)
    wide = feats // heads * heads_step
    lags = LEFT_SEGS * SEG_LEN // rows

    stats = jnp.concatenate([log_totals * LOG2E, out_dot], axis=1).T

    moved = {}
    for lag in range(1, lags + 1):
        moved[lag] = (shifted(query_rows, -lag), shifted(out_grad, -lag), shifted(stats, -lag))

    left_pad = 2 * half - REL_CLIP + half - SEG_LEN + 1
    padded = jnp.pad(bias_table, ((0, 0), (left_pad, 4 * half - left_pad - table_len)), mode="edge")
    chunks = padded.reshape(heads, 4, half)

    row_spec = pl.BlockSpec((rows, wide), lambda h: (0, h))
    stat_spec = pl.BlockSpec(stats.shape, lambda h: (0, 0))
    chunk_spec = pl.BlockSpec((heads_step, 4, half), lambda h: (h, 0, 0))
    tile_spec = pl.BlockSpec((heads_step, 3, half, half), lambda h: (h, 0, 0, 0))
    sq_spec = pl.BlockSpec((heads_step, rows, rows), lambda h: (h, 0, 0))
    rows_f32 = jax.ShapeDtypeStruct((rows, feats), F32)
    rows_b16 = jax.ShapeDtypeStruct((rows, feats), BF16)
    tab_shape = jax.ShapeDtypeStruct((heads, 4, half), F32)
    sq_shape = jax.ShapeDtypeStruct((heads, rows, rows), BF16)
    pair_flops = 2 * rows * rows * feats

    def cost(matmuls, size):
        return pl.CostEstimate(
            flops=matmuls * pair_flops, bytes_accessed=size, transcendentals=heads * rows * rows
        )

    tiles = pl.pallas_call(
        bias_kernel,
        grid=(heads,),
        in_specs=[pl.BlockSpec((1, 4, half), lambda h: (h, 0, 0))],
        out_specs=pl.BlockSpec((1, 3, half, half), lambda h: (h, 0, 0, 0)),
        out_shape=jax.ShapeDtypeStruct((heads, 3, half, half), F32),
        cost_estimate=cost(1, heads * 3 * half * half * 4),
        name="bias_tiles",
    )(chunks)

    base_specs = [row_spec] * 4 + [stat_spec, tile_spec, chunk_spec]
    body = functools.partial
    dq0, dk, dv, tab = pl.pallas_call(
        body(lag_kernel, 0, heads_step, heads, False),
        grid=grid,
        in_specs=base_specs,
        out_specs=[row_spec] * 3 + [chunk_spec],
        out_shape=[rows_f32] * 3 + [tab_shape],
        cost_estimate=cost(5, 8 * rows * feats),
        name="lag0",
    )(key_rows, value_rows, query_rows, out_grad, stats, tiles, chunks)

    dq2, dk, dv, tab = pl.pallas_call(
        body(lag_kernel, 2, heads_step, heads, False),
        grid=grid,
        in_specs=base_specs + [row_spec] * 2 + [chunk_spec],
        out_specs=[row_spec] * 3 + [chunk_spec],
        out_shape=[rows_b16] + [rows_f32] * 2 + [tab_shape],
        cost_estimate=cost(5, 8 * rows * feats),
        name="lag2",
    )(key_rows, value_rows, *moved[2], tiles, chunks, dk, dv, tab)
    back2 = shifted(dq2, 2)

    dq1, tab, weights, scores = pl.pallas_call(
        body(lag_kernel, 1, heads_step, heads, True),
        grid=grid,
        in_specs=base_specs + [chunk_spec],
        out_specs=[row_spec, chunk_spec, sq_spec, sq_spec],
        out_shape=[rows_b16, tab_shape, sq_shape, sq_shape],
        cost_estimate=cost(3, 8 * rows * feats),
        name="lag1",
    )(key_rows, value_rows, *moved[1], tiles, chunks, tab)
    back1 = shifted(dq1, 1)

    grad_key, grad_value = pl.pallas_call(
        body(close_kernel, heads_step),
        grid=grid,
        in_specs=[sq_spec, sq_spec] + [row_spec] * 4,
        out_specs=[row_spec] * 2,
        out_shape=[rows_b16] * 2,
        cost_estimate=cost(2, 8 * rows * feats),
        name="close",
    )(weights, scores, moved[1][0], moved[1][1], dk, dv)

    lines = all_sum(tab.reshape(heads, 4 * half))
    grad_table = jnp.concatenate(
        [
            lines[:, left_pad : left_pad + table_len - 1],
            jnp.sum(lines[:, left_pad + table_len - 1 :], axis=1, keepdims=True),
        ],
        axis=1,
    )
    grad_query = (dq0 + back1.astype(F32) + back2.astype(F32)).astype(BF16)
    return grad_query, grad_key, grad_value, grad_table


def solution(mesh):
    placed = (P(AXES, None),) * 6 + (P(),)
    return jax.shard_map(
        local,
        mesh=mesh,
        in_specs=placed,
        out_specs=(P(AXES, None),) * 3 + (P(),),
        check_vma=False,
    )
```

```python
import functools
import math

import jax
import jax.numpy as jnp
from jax import lax
from jax.experimental import pallas as pl
from jax.experimental.pallas import tpu as pltpu
from jax.sharding import PartitionSpec as P


SEG_LEN = 64
AXES = ("sp", "tp")
LOG2E = math.log2(math.e)
MASKED = -1e30
F32 = jnp.float32
BF16 = jnp.bfloat16
NT = (((1,), (1,)), ((), ()))
NN = (((1,), (0,)), ((), ()))


def shifted(block, distance):
    count = lax.axis_size(AXES)
    route = [(i - distance, i) for i in range(count) if 0 <= i - distance < count]
    return lax.ppermute(block, AXES, route)


def prime_radices(count):
    radices = []
    twos = 0
    while count % 2 == 0:
        count //= 2
        twos += 1
    while twos > 0:
        take = 2 if twos != 3 else 3
        take = min(take, twos)
        radices.append(2**take)
        twos -= take
    factor = 3
    while count > 1:
        while count % factor == 0:
            radices.append(factor)
            count //= factor
        factor += 2
    return radices


def pair_tree(parts):
    while len(parts) > 1:
        parts = [parts[i] + parts[i + 1] for i in range(0, len(parts), 2)]
    return parts[0]


def all_sum(part):
    count = lax.axis_size(AXES)
    me = lax.axis_index(AXES)
    stride = 1
    for radix in prime_radices(count):
        if radix & (radix - 1) == 0:
            parts = [part]
            for step in range(1, radix):
                route = [(i, i ^ (step * stride)) for i in range(count)]
                parts.append(lax.ppermute(part, AXES, route))
            part = pair_tree(parts)
        else:
            digit = (me // stride) % radix
            parts = [part]
            for step in range(1, radix):
                route = []
                for i in range(count):
                    d = (i // stride) % radix
                    route.append((i, i + (((d - step) % radix) - d) * stride))
                parts.append(lax.ppermute(part, AXES, route))
            total = jnp.zeros_like(part)
            for d in range(radix):
                value = parts[0]
                for step in range(1, radix):
                    value = jnp.where((digit + step) % radix == d, parts[step], value)
                total = total + value
            part = total
        stride *= radix
    return part


def prep_tiles(head_count, table_ref, chunk_ref, tile_ref):
    size = tile_ref.shape[2]
    table_len = table_ref.shape[1]
    span = chunk_ref.shape[1]
    pad = size - (SEG_LEN - 1)
    lane = lax.broadcasted_iota(jnp.int32, (head_count, span), 1)
    table = table_ref[...] * LOG2E
    first, last = table[:, :1], table[:, table_len - 1 :]
    wide = jnp.concatenate([table, jnp.zeros((head_count, span - table_len), F32)], axis=1)
    moved = pltpu.roll(wide, pad, 1)
    moved = jnp.where(lane < pad, first, jnp.where(lane >= pad + table_len, last, moved))
    chunk_ref[...] = moved
    row = lax.broadcasted_iota(jnp.int32, (size, size), 0)
    col = lax.broadcasted_iota(jnp.int32, (size, size), 1)

    @pl.loop(0, head_count)
    def _(head):
        rolled = []
        lines = chunk_ref[pl.ds(head, 1), :]
        for c in range(4):
            line = jnp.broadcast_to(lines[:, c * size : (c + 1) * size], (size, size))
            rolled.append(pltpu.roll(line, 0, 1, stride=1, stride_axis=0))
        for b in range(3):
            tile = jnp.where(col >= row, rolled[b + 1], rolled[b])
            if b == 0:
                tile = jnp.where((row // SEG_LEN) <= (col // SEG_LEN), tile, MASKED)
            tile_ref[head, b] = tile


def unroll_sum(tile):
    size = tile.shape[0]
    group = 8
    parts = []
    for start in range(0, size, group):
        part = tile[start : start + group, :]
        parts.append(part if start == 0 else pltpu.roll(part, size - start, 1))
    total = pair_tree(parts)
    row = lax.broadcasted_iota(jnp.int32, total.shape, 0)
    for bit in (1, 2, 4):
        total = jnp.where((row & bit) != 0, pltpu.roll(total, size - bit, 1), total)
    return jnp.sum(total, axis=0, keepdims=True)


def score_terms(lag, key, value, query, grad, log_row, dot_row, tiles, const, inv_root):
    rows = key.shape[0]
    half = rows // 2
    raw = lax.dot_general(key, query, NT, preferred_element_type=F32)
    wgt = lax.dot_general(value, grad, NT, preferred_element_type=F32)
    row = lax.broadcasted_iota(jnp.int32, (half, half), 0) // SEG_LEN
    col = lax.broadcasted_iota(jnp.int32, (half, half), 1) // SEG_LEN
    acc = [None, None, None, None]
    w_rows, s_rows = [], []
    for r in range(2):
        w_cols, s_cols = [], []
        for c in range(2):
            if (lag == 0 and r > c) or (lag == 2 and c > r):
                w_cols.append(jnp.zeros((half, half), BF16))
                s_cols.append(jnp.zeros((half, half), BF16))
                continue
            rs, cs = slice(r * half, (r + 1) * half), slice(c * half, (c + 1) * half)
            level = min(2 * lag + c - r, 3)
            lrow = log_row[:, cs]
            bias = const - lrow if level == 3 else tiles[level] - lrow
            weight = jnp.exp2(raw[rs, cs] * (inv_root * LOG2E) + bias)
            if lag == 2 and r == c:
                weight = jnp.where(col <= row, weight, 0.0)
            score = weight * (wgt[rs, cs] - dot_row[:, cs])
            acc[level] = score if acc[level] is None else acc[level] + score
            w_cols.append(weight.astype(BF16))
            s_cols.append(score.astype(BF16))
        w_rows.append(jnp.concatenate(w_cols, axis=1))
        s_rows.append(jnp.concatenate(s_cols, axis=1))
    return jnp.concatenate(w_rows, axis=0), jnp.concatenate(s_rows, axis=0), acc


def table_lines(acc, size):
    row = lax.broadcasted_iota(jnp.int32, (size, size), 0)
    col = lax.broadcasted_iota(jnp.int32, (size, size), 1)
    zero = jnp.zeros((size, size), F32)
    lines = []
    for c in range(4):
        upper = acc[c - 1] if c > 0 else None
        lower = acc[c] if c < 3 else None
        line = None
        if upper is not None or lower is not None:
            mixed = jnp.where(
                col >= row,
                zero if upper is None else upper,
                zero if lower is None else lower,
            )
            line = unroll_sum(mixed)
        if c == 3 and acc[3] is not None:
            extra = jnp.sum(acc[3], axis=0, keepdims=True)
            line = extra if line is None else line + extra
        lines.append(line)
    return lines


def lag_kernel(lag, heads_step, head_count, *refs):
    if lag == 0:
        (k_ref, v_ref, q_ref, g_ref, st_ref, table_ref,
         dq_ref, dk_ref, dv_ref, tab_ref, kt_ref, tile_ref, chunk_ref) = refs
        prep_tiles(head_count, table_ref, chunk_ref, tile_ref)
    elif lag == 2:
        (k_ref, v_ref, q_ref, g_ref, st_ref, kt_ref, tile_ref, chunk_ref, dk_in, dv_in, tab_in,
         dq_ref, dk_ref, dv_ref, tab_ref) = refs
    else:
        (k_ref, v_ref, q_ref, g_ref, st_ref, kt_ref, tile_ref, chunk_ref, tab_in,
         dq_ref, tab_ref, w_ref, s_ref) = refs
    size = tile_ref.shape[2]
    head_dim = k_ref.shape[1] // head_count
    inv_root = head_dim ** (-0.5)

    @pl.loop(0, head_count // heads_step)
    def _(step):
        for i in range(heads_step):
            head = step * heads_step + i
            cols = pl.ds(pl.multiple_of(head * head_dim, head_dim), head_dim)
            key, value, query, grad = k_ref[:, cols], v_ref[:, cols], q_ref[:, cols], g_ref[:, cols]
            log_row = st_ref[pl.ds(head, 1), :]
            dot_row = st_ref[pl.ds(head + head_count, 1), :]
            const = chunk_ref[pl.ds(head, 1), :][:, 3 * size :]
            tiles = [None if lag == 2 else tile_ref[head, b] for b in range(3)]
            weights, scores, acc = score_terms(
                lag, key, value, query, grad, log_row, dot_row, tiles, const, inv_root
            )
            if lag == 0:
                turned = key.T
                kt_ref[cols, :] = turned
            else:
                turned = kt_ref[cols, :]
            dq = lax.dot_general(turned, scores, NN, preferred_element_type=F32) * inv_root
            dq_ref[cols, :] = dq.astype(dq_ref.dtype)
            lines = [
                jnp.zeros((1, size), F32) if line is None else line
                for line in table_lines(acc, size)
            ]
            lines = jnp.concatenate(lines, axis=1)
            row_at = pl.ds(head, 1)
            tab_ref[row_at, :] = lines if lag == 0 else tab_in[row_at, :] + lines
            if lag == 1:
                w_ref[head] = weights
                s_ref[head] = scores
            else:
                dk = lax.dot_general(scores, query, NN, preferred_element_type=F32)
                dv = lax.dot_general(weights, grad, NN, preferred_element_type=F32)
                dk_ref[:, cols] = dk if lag == 0 else dk + dk_in[:, cols]
                dv_ref[:, cols] = dv if lag == 0 else dv + dv_in[:, cols]


def close_kernel(heads_step, w_ref, s_ref, q_ref, g_ref, dk_in, dv_in, dk_ref, dv_ref):
    head_count = w_ref.shape[0]
    head_dim = q_ref.shape[1] // head_count
    inv_root = head_dim ** (-0.5)

    @pl.loop(0, head_count // heads_step)
    def _(step):
        for i in range(heads_step):
            head = step * heads_step + i
            cols = pl.ds(pl.multiple_of(head * head_dim, head_dim), head_dim)
            dk = lax.dot_general(s_ref[head], q_ref[:, cols], NN, preferred_element_type=F32)
            dv = lax.dot_general(w_ref[head], g_ref[:, cols], NN, preferred_element_type=F32)
            dk_ref[:, cols] = ((dk + dk_in[:, cols]) * inv_root).astype(BF16)
            dv_ref[:, cols] = (dv + dv_in[:, cols]).astype(BF16)


def query_kernel(heads_step, head_count, dq_ref, one_ref, two_ref, out_ref):
    head_dim = dq_ref.shape[0] // head_count

    @pl.loop(0, head_count // heads_step)
    def _(step):
        for i in range(heads_step):
            cols = pl.ds(pl.multiple_of((step * heads_step + i) * head_dim, head_dim), head_dim)
            total = dq_ref[cols, :] + one_ref[cols, :].astype(F32) + two_ref[cols, :].astype(F32)
            out_ref[:, cols] = total.T.astype(BF16)


def local(query_rows, key_rows, value_rows, out_grad, log_totals, out_dot, bias_table):
    rows, feats = query_rows.shape
    heads = log_totals.shape[1]
    table_len = bias_table.shape[1]
    half = rows // 2
    pair_flops = 2 * rows * rows * feats

    def cost(matmuls):
        return pl.CostEstimate(
            flops=matmuls * pair_flops,
            bytes_accessed=8 * rows * feats,
            transcendentals=heads * rows * rows,
        )

    def call(body, matmuls, outs, *args):
        return pl.pallas_call(
            body,
            in_specs=[pl.BlockSpec(memory_space=pltpu.VMEM)] * len(args),
            out_specs=[pl.BlockSpec(memory_space=pltpu.VMEM)] * len(outs),
            out_shape=outs,
            cost_estimate=cost(matmuls),
            compiler_params=pltpu.CompilerParams(vmem_limit_bytes=16 * 2**20),
        )(*args)

    moved = {}
    stats = jnp.concatenate([log_totals * LOG2E, out_dot], axis=1).T
    for lag in (1, 2):
        parts = []
        for part in (query_rows, out_grad, stats):
            parts.append(shifted(part, -lag))
        moved[lag] = parts

    rows_f32 = pltpu.VMEM((rows, feats), F32)
    rows_b16 = pltpu.VMEM((rows, feats), BF16)
    turn_f32 = pltpu.VMEM((feats, rows), F32)
    turn_b16 = pltpu.VMEM((feats, rows), BF16)
    tab_shape = pltpu.VMEM((heads, 4 * half), F32)
    sq_shape = pltpu.VMEM((heads, rows, rows), BF16)
    tile_shape = pltpu.VMEM((heads, 3, half, half), F32)

    body = functools.partial
    dq0, dk, dv, tab, turned, tiles, chunks = call(
        body(lag_kernel, 0, 2, heads), 5,
        [turn_f32, rows_f32, rows_f32, tab_shape, turn_b16, tile_shape, tab_shape],
        key_rows, value_rows, query_rows, out_grad, stats, bias_table,
    )
    dq2, dk, dv, tab = call(
        body(lag_kernel, 2, 2, heads), 5,
        [turn_b16, rows_f32, rows_f32, tab_shape],
        key_rows, value_rows, *moved[2], turned, tiles, chunks, dk, dv, tab,
    )
    back2 = shifted(dq2, 2)
    dq1, tab, weights, scores = call(
        body(lag_kernel, 1, 2, heads), 3,
        [turn_b16, tab_shape, sq_shape, sq_shape],
        key_rows, value_rows, *moved[1], turned, tiles, chunks, tab,
    )
    back1 = shifted(dq1, 1)
    lines = all_sum(tab)
    out_shape = jax.ShapeDtypeStruct((rows, feats), BF16)
    grad_key, grad_value = call(
        body(close_kernel, 2), 2, [out_shape, out_shape],
        weights, scores, moved[1][0], moved[1][1], dk, dv,
    )
    grad_query, = call(body(query_kernel, 2, heads), 1, [out_shape], dq0, back1, back2)
    start = half - (SEG_LEN - 1)
    grad_table = jnp.concatenate(
        [
            lines[:, start : start + table_len - 1],
            jnp.sum(lines[:, start + table_len - 1 :], axis=1, keepdims=True),
        ],
        axis=1,
    )
    return grad_query, grad_key, grad_value, grad_table


def solution(mesh):
    placed = (P(AXES, None),) * 6 + (P(),)
    return jax.shard_map(
        local,
        mesh=mesh,
        in_specs=placed,
        out_specs=(P(AXES, None),) * 3 + (P(),),
        check_vma=False,
    )
```

```python
import functools
import math

import jax
import jax.numpy as jnp
from jax import lax
from jax.experimental import pallas as pl
from jax.experimental.pallas import tpu as pltpu
from jax.sharding import PartitionSpec as P


SEG_LEN = 64
AXES = ("sp", "tp")
LOG2E = math.log2(math.e)
MASKED = -1e30
PACK = 128
F32 = jnp.float32
BF16 = jnp.bfloat16
NT = (((1,), (1,)), ((), ()))
NN = (((1,), (0,)), ((), ()))


def shifted(block, distance):
    count = lax.axis_size(AXES)
    route = [(i - distance, i) for i in range(count) if 0 <= i - distance < count]
    return lax.ppermute(block, AXES, route)


def prime_radices(count):
    radices = []
    twos = 0
    while count % 2 == 0:
        count //= 2
        twos += 1
    while twos > 0:
        take = 1 if not radices else min(2, twos)
        radices.append(2**take)
        twos -= take
    factor = 3
    while count > 1:
        while count % factor == 0:
            radices.append(factor)
            count //= factor
        factor += 2
    return radices


def pair_tree(parts):
    while len(parts) > 1:
        parts = [parts[i] + parts[i + 1] for i in range(0, len(parts), 2)]
    return parts[0]


def all_sum(part):
    count = lax.axis_size(AXES)
    me = lax.axis_index(AXES)
    stride = 1
    for radix in prime_radices(count):
        if radix & (radix - 1) == 0:
            parts = [part]
            for step in range(1, radix):
                route = [(i, i ^ (step * stride)) for i in range(count)]
                parts.append(lax.ppermute(part, AXES, route))
            part = pair_tree(parts)
        else:
            digit = (me // stride) % radix
            parts = [part]
            for step in range(1, radix):
                route = []
                for i in range(count):
                    d = (i // stride) % radix
                    route.append((i, i + (((d - step) % radix) - d) * stride))
                parts.append(lax.ppermute(part, AXES, route))
            total = jnp.zeros_like(part)
            for d in range(radix):
                value = parts[0]
                for step in range(1, radix):
                    value = jnp.where((digit + step) % radix == d, parts[step], value)
                total = total + value
            part = total
        stride *= radix
    return part


def prep_tiles(head_count, table_ref, chunk_ref, tile_ref):
    size = tile_ref.shape[2]
    table_len = table_ref.shape[1]
    span = chunk_ref.shape[1]
    pad = size - (SEG_LEN - 1)
    lane = lax.broadcasted_iota(jnp.int32, (head_count, span), 1)
    table = table_ref[...] * LOG2E
    first, last = table[:, :1], table[:, table_len - 1 :]
    wide = jnp.concatenate([table, jnp.zeros((head_count, span - table_len), F32)], axis=1)
    moved = pltpu.roll(wide, pad, 1)
    moved = jnp.where(lane < pad, first, jnp.where(lane >= pad + table_len, last, moved))
    chunk_ref[...] = moved
    row = lax.broadcasted_iota(jnp.int32, (size, size), 0)
    col = lax.broadcasted_iota(jnp.int32, (size, size), 1)

    @pl.loop(0, head_count)
    def _(head):
        rolled = []
        lines = chunk_ref[pl.ds(head, 1), :]
        for c in range(4):
            line = jnp.broadcast_to(lines[:, c * size : (c + 1) * size], (size, size))
            rolled.append(pltpu.roll(line, 0, 1, stride=1, stride_axis=0))
        for b in range(3):
            tile = jnp.where(col >= row, rolled[b + 1], rolled[b])
            if b == 0:
                tile = jnp.where((row // SEG_LEN) <= (col // SEG_LEN), tile, MASKED)
            tile_ref[head, b] = tile


def unroll_sum(tile):
    size = tile.shape[0]
    group = 8
    parts = []
    for start in range(0, size, group):
        part = tile[start : start + group, :]
        parts.append(part if start == 0 else pltpu.roll(part, size - start, 1))
    total = pair_tree(parts)
    row = lax.broadcasted_iota(jnp.int32, total.shape, 0)
    for bit in (1, 2, 4):
        total = jnp.where((row & bit) != 0, pltpu.roll(total, size - bit, 1), total)
    return jnp.sum(total, axis=0, keepdims=True)


def score_terms(lag, key, value, query, grad, log_row, dot_row, tiles, const, inv_root):
    rows = key.shape[0]
    half = rows // 2
    raw = lax.dot_general(key, query, NT, preferred_element_type=F32)
    wgt = lax.dot_general(value, grad, NT, preferred_element_type=F32)
    row = lax.broadcasted_iota(jnp.int32, (half, half), 0) // SEG_LEN
    col = lax.broadcasted_iota(jnp.int32, (half, half), 1) // SEG_LEN
    acc = [None, None, None, None]
    w_rows, s_rows = [], []
    for r in range(2):
        w_cols, s_cols = [], []
        for c in range(2):
            if (lag == 0 and r > c) or (lag == 2 and c > r):
                w_cols.append(jnp.zeros((half, half), BF16))
                s_cols.append(jnp.zeros((half, half), BF16))
                continue
            rs, cs = slice(r * half, (r + 1) * half), slice(c * half, (c + 1) * half)
            level = min(2 * lag + c - r, 3)
            lrow = log_row[:, cs]
            bias = const - lrow if level == 3 else tiles[level] - lrow
            weight = jnp.exp2(raw[rs, cs] * (inv_root * LOG2E) + bias)
            if lag == 2 and r == c:
                weight = jnp.where(col <= row, weight, 0.0)
            score = weight * (wgt[rs, cs] - dot_row[:, cs])
            acc[level] = score if acc[level] is None else acc[level] + score
            w_cols.append(weight.astype(BF16))
            s_cols.append(score.astype(BF16))
        w_rows.append(jnp.concatenate(w_cols, axis=1))
        s_rows.append(jnp.concatenate(s_cols, axis=1))
    return jnp.concatenate(w_rows, axis=0), jnp.concatenate(s_rows, axis=0), acc


def table_lines(acc, size):
    row = lax.broadcasted_iota(jnp.int32, (size, size), 0)
    col = lax.broadcasted_iota(jnp.int32, (size, size), 1)
    zero = jnp.zeros((size, size), F32)
    lines = []
    for c in range(4):
        upper = acc[c - 1] if c > 0 else None
        lower = acc[c] if c < 3 else None
        line = None
        if upper is not None or lower is not None:
            mixed = jnp.where(
                col >= row,
                zero if upper is None else upper,
                zero if lower is None else lower,
            )
            line = unroll_sum(mixed)
        if c == 3 and acc[3] is not None:
            extra = jnp.sum(acc[3], axis=0, keepdims=True)
            line = extra if line is None else line + extra
        lines.append(line)
    return lines


def read_stats(g_ref, stat_ref):
    count = stat_ref.shape[0]
    packed = g_ref[:, g_ref.shape[1] - PACK :].astype(F32).T
    stat_ref[...] = packed[:count] + packed[count : 2 * count] + packed[2 * count : 3 * count]


def fold_table(lines, table_len, size):
    pad = size - (SEG_LEN - 1)
    lane = lax.broadcasted_iota(jnp.int32, lines.shape, 1)
    tail = jnp.sum(jnp.where(lane >= pad + table_len - 1, lines, 0.0), axis=1, keepdims=True)
    moved = pltpu.roll(lines, lines.shape[1] - pad, 1)[:, :table_len]
    lane = lax.broadcasted_iota(jnp.int32, moved.shape, 1)
    return jnp.where(lane == table_len - 1, tail, moved)


def lag_kernel(lag, heads_step, head_count, *refs):
    copies = []
    if lag == 0:
        (k_hbm, v_hbm, q_hbm, g_ref, table_hbm,
         dq_ref, dk_ref, dv_ref, tab_ref, kt_ref, tile_ref, chunk_ref, k_ref, v_ref,
         q_ref, table_ref, stat_ref, sems) = refs
        pairs = ((table_hbm, table_ref), (k_hbm, k_ref), (v_hbm, v_ref), (q_hbm, q_ref))
        for i, (source, target) in enumerate(pairs):
            copies.append(pltpu.make_async_copy(source, target, sems.at[i]))
            copies[-1].start()
        read_stats(g_ref, stat_ref)
        copies[0].wait()
        prep_tiles(head_count, table_ref, chunk_ref, tile_ref)
        for copy in copies[1:]:
            copy.wait()
    elif lag == 2:
        (k_ref, v_ref, q_ref, g_ref, kt_ref, tile_ref, chunk_ref, dk_in, dv_in, tab_in,
         dq_ref, dk_ref, dv_ref, tab_ref, stat_ref) = refs
        read_stats(g_ref, stat_ref)
    else:
        (k_ref, v_ref, q_ref, g_ref, kt_ref, tile_ref, chunk_ref, tab_in,
         dq_ref, out_tab_ref, w_ref, s_ref, tab_ref, stat_ref) = refs
        read_stats(g_ref, stat_ref)
    size = tile_ref.shape[2]
    head_dim = k_ref.shape[1] // head_count
    inv_root = head_dim ** (-0.5)

    @pl.loop(0, head_count // heads_step)
    def _(step):
        for i in range(heads_step):
            head = step * heads_step + i
            cols = pl.ds(pl.multiple_of(head * head_dim, head_dim), head_dim)
            key, value, query, grad = k_ref[:, cols], v_ref[:, cols], q_ref[:, cols], g_ref[:, cols]
            log_row = stat_ref[pl.ds(head, 1), :]
            dot_row = stat_ref[pl.ds(head + head_count, 1), :]
            const = chunk_ref[pl.ds(head, 1), :][:, 3 * size :]
            tiles = [None if lag == 2 else tile_ref[head, b] for b in range(3)]
            weights, scores, acc = score_terms(
                lag, key, value, query, grad, log_row, dot_row, tiles, const, inv_root
            )
            if lag == 0:
                turned = key.T
                kt_ref[cols, :] = turned
            else:
                turned = kt_ref[cols, :]
            dq = lax.dot_general(turned, scores, NN, preferred_element_type=F32) * inv_root
            dq_ref[cols, :] = dq.astype(dq_ref.dtype)
            lines = [
                jnp.zeros((1, size), F32) if line is None else line
                for line in table_lines(acc, size)
            ]
            lines = jnp.concatenate(lines, axis=1)
            row_at = pl.ds(head, 1)
            tab_ref[row_at, :] = lines if lag == 0 else tab_in[row_at, :] + lines
            if lag == 1:
                w_ref[head] = weights
                s_ref[head] = scores
            else:
                dk = lax.dot_general(scores, query, NN, preferred_element_type=F32)
                dv = lax.dot_general(weights, grad, NN, preferred_element_type=F32)
                dk_ref[:, cols] = dk if lag == 0 else dk + dk_in[:, cols]
                dv_ref[:, cols] = dv if lag == 0 else dv + dv_in[:, cols]

    if lag == 1:
        out_tab_ref[...] = fold_table(tab_ref[...], out_tab_ref.shape[1], size)


def close_kernel(heads_step, scaled, w_ref, x_ref, part_ref, out_ref):
    head_count = w_ref.shape[0]
    head_dim = out_ref.shape[1] // head_count
    scale = head_dim ** (-0.5) if scaled else 1.0

    @pl.loop(0, head_count // heads_step)
    def _(step):
        for i in range(heads_step):
            head = step * heads_step + i
            cols = pl.ds(pl.multiple_of(head * head_dim, head_dim), head_dim)
            total = lax.dot_general(w_ref[head], x_ref[:, cols], NN, preferred_element_type=F32)
            out_ref[:, cols] = ((total + part_ref[:, cols]) * scale).astype(BF16)


def query_kernel(heads_step, head_count, dq_ref, one_ref, two_ref, out_ref):
    head_dim = dq_ref.shape[0] // head_count

    @pl.loop(0, head_count // heads_step)
    def _(step):
        for i in range(heads_step):
            cols = pl.ds(pl.multiple_of((step * heads_step + i) * head_dim, head_dim), head_dim)
            total = dq_ref[cols, :] + one_ref[cols, :].astype(F32) + two_ref[cols, :].astype(F32)
            out_ref[:, cols] = total.T.astype(BF16)


def packed_grads(out_grad, log_totals, out_dot):
    stats = jnp.concatenate([log_totals * LOG2E, out_dot], axis=1)
    high = lax.reduce_precision(stats, 8, 7)
    rest = stats - high
    mid = lax.reduce_precision(rest, 8, 7)
    terms = jnp.concatenate([high, mid, rest - mid], axis=1).astype(BF16)
    terms = jnp.pad(terms, ((0, 0), (0, PACK - terms.shape[1])))
    return jnp.concatenate([out_grad, terms], axis=1)


def local(query_rows, key_rows, value_rows, out_grad, log_totals, out_dot, bias_table):
    rows, feats = query_rows.shape
    heads = log_totals.shape[1]
    table_len = bias_table.shape[1]
    half = rows // 2
    pair_flops = 2 * rows * rows * feats
    vmem = pl.BlockSpec(memory_space=pltpu.VMEM)
    hbm = pl.BlockSpec(memory_space=pltpu.HBM)

    def cost(matmuls):
        return pl.CostEstimate(
            flops=matmuls * pair_flops,
            bytes_accessed=8 * rows * feats,
            transcendentals=heads * rows * rows,
        )

    def call(body, matmuls, outs, args, scratch=(), specs=None):
        return pl.pallas_call(
            body,
            in_specs=[vmem] * len(args) if specs is None else specs,
            out_specs=[vmem] * len(outs),
            out_shape=outs,
            scratch_shapes=list(scratch),
            cost_estimate=cost(matmuls),
            compiler_params=pltpu.CompilerParams(vmem_limit_bytes=16 * 2**20),
        )(*args)

    grads = packed_grads(out_grad, log_totals, out_dot)
    moved = {}
    for lag in (1, 2):
        parts = []
        for part in (query_rows, grads):
            parts.append(shifted(part, -lag))
        moved[lag] = parts

    rows_f32 = pltpu.VMEM((rows, feats), F32)
    rows_b16 = pltpu.VMEM((rows, feats), BF16)
    turn_f32 = pltpu.VMEM((feats, rows), F32)
    turn_b16 = pltpu.VMEM((feats, rows), BF16)
    wide_tab = pltpu.VMEM((heads, 4 * half), F32)
    table_shape = pltpu.VMEM((heads, table_len), F32)
    sq_shape = pltpu.VMEM((heads, rows, rows), BF16)
    tile_shape = pltpu.VMEM((heads, 3, half, half), F32)
    stat_shape = pltpu.VMEM((2 * heads, rows), F32)
    out_shape = jax.ShapeDtypeStruct((rows, feats), BF16)

    body = functools.partial
    dq0, dk, dv, tab, turned, tiles, chunks, keys, values = call(
        body(lag_kernel, 0, 2, heads), 5,
        [turn_f32, rows_f32, rows_f32, wide_tab, turn_b16, tile_shape, wide_tab,
         rows_b16, rows_b16],
        (key_rows, value_rows, query_rows, grads, bias_table),
        (rows_b16, table_shape, stat_shape, pltpu.SemaphoreType.DMA((4,))),
        [hbm, hbm, hbm, vmem, hbm],
    )
    dq2, dk, dv, tab = call(
        body(lag_kernel, 2, 2, heads), 5,
        [turn_b16, rows_f32, rows_f32, wide_tab],
        (keys, values, *moved[2], turned, tiles, chunks, dk, dv, tab),
        (stat_shape,),
    )
    back2 = shifted(dq2, 2)
    dq1, table_part, weights, scores = call(
        body(lag_kernel, 1, 2, heads), 3,
        [turn_b16, table_shape, sq_shape, sq_shape],
        (keys, values, *moved[1], turned, tiles, chunks, tab),
        (wide_tab, stat_shape),
    )
    back1 = shifted(dq1, 1)
    grad_table = all_sum(table_part)
    grad_key, = call(
        body(close_kernel, 2, True), 1, [out_shape],
        (scores, moved[1][0], dk),
    )
    grad_value, = call(
        body(close_kernel, 2, False), 1, [out_shape],
        (weights, moved[1][1], dv),
    )
    grad_query, = call(body(query_kernel, 2, heads), 1, [out_shape], (dq0, back1, back2))
    return grad_query, grad_key, grad_value, grad_table


def solution(mesh):
    placed = (P(AXES, None),) * 6 + (P(),)
    return jax.shard_map(
        local,
        mesh=mesh,
        in_specs=placed,
        out_specs=(P(AXES, None),) * 3 + (P(),),
        check_vma=False,
    )
```

```python
import functools
import math

import jax
import jax.numpy as jnp
from jax import lax
from jax.experimental import pallas as pl
from jax.experimental.pallas import tpu as pltpu
from jax.sharding import PartitionSpec as P


SEG_LEN = 64
AXES = ("sp", "tp")
LOG2E = math.log2(math.e)
MASKED = -1e30
TERMS = 3
ROUND_ORDER = ((1,), (3, 4), (0, 2))
F32 = jnp.float32
BF16 = jnp.bfloat16
NT = (((1,), (1,)), ((), ()))
NN = (((1,), (0,)), ((), ()))


def shifted(block, distance):
    count = lax.axis_size(AXES)
    route = [(i - distance, i) for i in range(count) if 0 <= i - distance < count]
    return lax.ppermute(block, AXES, route)


def pair_tree(parts):
    while len(parts) > 1:
        parts = [parts[i] + parts[i + 1] for i in range(0, len(parts), 2)]
    return parts[0]


def table_rounds(count):
    twos = []
    stride = 1
    while count % (2 * stride) == 0:
        twos.append(stride)
        stride *= 2
    order = ROUND_ORDER
    rounds = [tuple(twos[d] for d in digits if d < len(twos)) for digits in order]
    used = sum(len(digits) for digits in order)
    rounds += [(twos[d],) for d in range(used, len(twos))]
    odd = []
    rest, factor = count // stride, 3
    while rest > 1:
        while rest % factor == 0:
            odd.append((stride, factor))
            stride *= factor
            rest //= factor
        factor += 2
    return [r for r in rounds if r], odd


def all_sum(part):
    count = lax.axis_size(AXES)
    me = lax.axis_index(AXES)
    binary, odd = table_rounds(count)
    for strides in binary:
        masks = [0]
        for stride in strides:
            masks += [mask ^ stride for mask in masks]
        parts = [part]
        for mask in masks[1:]:
            parts.append(lax.ppermute(part, AXES, [(i, i ^ mask) for i in range(count)]))
        part = pair_tree(parts)
    for stride, radix in odd:
        digit = (me // stride) % radix
        parts = [part]
        for step in range(1, radix):
            route = []
            for i in range(count):
                d = (i // stride) % radix
                route.append((i, i + (((d - step) % radix) - d) * stride))
            parts.append(lax.ppermute(part, AXES, route))
        total = jnp.zeros_like(part)
        for d in range(radix):
            value = parts[0]
            for step in range(1, radix):
                value = jnp.where((digit + step) % radix == d, parts[step], value)
            total = total + value
        part = total
    return part


def prep_tiles(head_count, table_ref, chunk_ref, tile_ref):
    size = tile_ref.shape[2]
    table_len = table_ref.shape[1]
    span = chunk_ref.shape[1]
    pad = size - (SEG_LEN - 1)
    lane = lax.broadcasted_iota(jnp.int32, (head_count, span), 1)
    table = table_ref[...] * LOG2E
    first, last = table[:, :1], table[:, table_len - 1 :]
    wide = jnp.concatenate([table, jnp.zeros((head_count, span - table_len), F32)], axis=1)
    moved = pltpu.roll(wide, pad, 1)
    moved = jnp.where(lane < pad, first, jnp.where(lane >= pad + table_len, last, moved))
    chunk_ref[...] = moved
    row = lax.broadcasted_iota(jnp.int32, (size, size), 0)
    col = lax.broadcasted_iota(jnp.int32, (size, size), 1)

    @pl.loop(0, head_count)
    def _(head):
        rolled = []
        lines = chunk_ref[pl.ds(head, 1), :]
        for c in range(4):
            line = jnp.broadcast_to(lines[:, c * size : (c + 1) * size], (size, size))
            rolled.append(pltpu.roll(line, 0, 1, stride=1, stride_axis=0))
        for b in range(3):
            tile = jnp.where(col >= row, rolled[b + 1], rolled[b])
            if b == 0:
                tile = jnp.where((row // SEG_LEN) <= (col // SEG_LEN), tile, MASKED)
            tile_ref[head, b] = tile


def unroll_sum(tile):
    size = tile.shape[0]
    group = 8
    parts = []
    for start in range(0, size, group):
        part = tile[start : start + group, :]
        parts.append(part if start == 0 else pltpu.roll(part, size - start, 1))
    total = pair_tree(parts)
    row = lax.broadcasted_iota(jnp.int32, total.shape, 0)
    for bit in (1, 2, 4):
        total = jnp.where((row & bit) != 0, pltpu.roll(total, size - bit, 1), total)
    return jnp.sum(total, axis=0, keepdims=True)


def score_terms(lag, key, value, query, grad, log_row, dot_row, tiles, const, inv_root):
    rows = key.shape[0]
    half = rows // 2
    raw = lax.dot_general(key, query, NT, preferred_element_type=F32)
    wgt = lax.dot_general(value, grad, NT, preferred_element_type=F32)
    row = lax.broadcasted_iota(jnp.int32, (half, half), 0) // SEG_LEN
    col = lax.broadcasted_iota(jnp.int32, (half, half), 1) // SEG_LEN
    acc = [None, None, None, None]
    w_rows, s_rows = [], []
    for r in range(2):
        w_cols, s_cols = [], []
        for c in range(2):
            if (lag == 0 and r > c) or (lag == 2 and c > r):
                w_cols.append(jnp.zeros((half, half), BF16))
                s_cols.append(jnp.zeros((half, half), BF16))
                continue
            rs, cs = slice(r * half, (r + 1) * half), slice(c * half, (c + 1) * half)
            level = min(2 * lag + c - r, 3)
            lrow = log_row[:, cs]
            bias = const - lrow if level == 3 else tiles[level] - lrow
            weight = jnp.exp2(raw[rs, cs] * (inv_root * LOG2E) + bias)
            if lag == 2 and r == c:
                weight = jnp.where(col <= row, weight, 0.0)
            score = weight * (wgt[rs, cs] - dot_row[:, cs])
            acc[level] = score if acc[level] is None else acc[level] + score
            w_cols.append(weight.astype(BF16))
            s_cols.append(score.astype(BF16))
        w_rows.append(jnp.concatenate(w_cols, axis=1))
        s_rows.append(jnp.concatenate(s_cols, axis=1))
    return jnp.concatenate(w_rows, axis=0), jnp.concatenate(s_rows, axis=0), acc


def table_lines(acc, size):
    row = lax.broadcasted_iota(jnp.int32, (size, size), 0)
    col = lax.broadcasted_iota(jnp.int32, (size, size), 1)
    zero = jnp.zeros((size, size), F32)
    lines = []
    for c in range(4):
        upper = acc[c - 1] if c > 0 else None
        lower = acc[c] if c < 3 else None
        line = None
        if upper is not None or lower is not None:
            mixed = jnp.where(
                col >= row,
                zero if upper is None else upper,
                zero if lower is None else lower,
            )
            line = unroll_sum(mixed)
        if c == 3 and acc[3] is not None:
            extra = jnp.sum(acc[3], axis=0, keepdims=True)
            line = extra if line is None else line + extra
        lines.append(line)
    return lines


def fold_table(lines, table_len, size):
    pad = size - (SEG_LEN - 1)
    lane = lax.broadcasted_iota(jnp.int32, lines.shape, 1)
    tail = jnp.sum(jnp.where(lane >= pad + table_len - 1, lines, 0.0), axis=1, keepdims=True)
    moved = pltpu.roll(lines, lines.shape[1] - pad, 1)[:, :table_len]
    lane = lax.broadcasted_iota(jnp.int32, moved.shape, 1)
    return jnp.where(lane == table_len - 1, tail, moved)


def pack_height(count, rows, width):
    lines = -(-count * TERMS * rows // width)
    return -(-lines // 8) * 8


def pack_lines(stats, width):
    count, rows = stats.shape
    high = stats.astype(BF16).astype(F32)
    rest = stats - high
    mid = rest.astype(BF16).astype(F32)
    terms = (high, mid, rest - mid)
    per_row = width // rows
    lines = []
    for line in range(pack_height(count, rows, width)):
        pieces = []
        for b in range(line * per_row, (line + 1) * per_row):
            if b < count * TERMS:
                pieces.append(terms[b // count][b % count : b % count + 1, :])
            else:
                pieces.append(jnp.zeros((1, rows), F32))
        lines.append(jnp.concatenate(pieces, axis=1))
    return jnp.concatenate(lines, axis=0).astype(BF16)


def unpack_lines(pack_ref, stat_ref):
    count, rows = stat_ref.shape
    per_row = pack_ref.shape[1] // rows
    packed = pack_ref[rows:, :].astype(F32)
    for i in range(count):
        total = None
        for term in range(TERMS):
            line, at = divmod(term * count + i, per_row)
            piece = packed[line : line + 1, at * rows : (at + 1) * rows]
            total = piece if total is None else total + piece
        stat_ref[i : i + 1, :] = total


def prep_kernel(g_hbm, log_hbm, dot_hbm, far_ref, first_ref, second_ref, stat_ref,
                log_ref, dot_ref, sems):
    rows, feats = g_hbm.shape
    cut = first_ref.shape[1]
    moves = (
        (log_hbm, log_ref),
        (dot_hbm, dot_ref),
        (g_hbm, far_ref.at[pl.ds(0, rows), :]),
        (g_hbm.at[:, pl.ds(0, cut)], first_ref.at[pl.ds(0, rows), :]),
        (g_hbm.at[:, pl.ds(cut, feats - cut)], second_ref),
    )
    copies = []
    for i, (origin, target) in enumerate(moves):
        copies.append(pltpu.make_async_copy(origin, target, sems.at[i]))
        copies[-1].start()
    for copy in copies[:2]:
        copy.wait()
    stats = jnp.concatenate([log_ref[...] * LOG2E, dot_ref[...]], axis=0)
    stat_ref[...] = stats
    first_ref[rows:, :] = pack_lines(stats, first_ref.shape[1])
    far_ref[rows:, :] = pack_lines(stats, far_ref.shape[1])
    for copy in copies[2:]:
        copy.wait()


def lag_kernel(lag, first_head, last_head, heads_step, head_count, *refs):
    if lag == 0:
        (k_hbm, v_hbm, q_hbm, table_hbm, g_ref, stat_ref,
         dq_ref, dk_ref, dv_ref, tab_ref, kt_ref, tile_ref, chunk_ref, k_ref, v_ref,
         q_ref, table_ref, sems) = refs
        pairs = ((table_hbm, table_ref), (k_hbm, k_ref), (v_hbm, v_ref), (q_hbm, q_ref))
        copies = []
        for i, (source, target) in enumerate(pairs):
            copies.append(pltpu.make_async_copy(source, target, sems.at[i]))
            copies[-1].start()
        copies[0].wait()
        prep_tiles(head_count, table_ref, chunk_ref, tile_ref)
        for copy in copies[1:]:
            copy.wait()
    elif lag == 2:
        (k_ref, v_ref, kt_ref, tile_ref, chunk_ref, dk_in, dv_in, tab_in, q_ref, g_ref,
         dk_ref, dv_ref, tab_ref, dq_ref, stat_ref) = refs
        unpack_lines(g_ref, stat_ref)
    elif first_head == 0:
        (k_ref, v_ref, kt_ref, tile_ref, chunk_ref, dk_in, dv_in, tab_in, q_ref, g_ref,
         dk_ref, dv_ref, tab_ref, dq_ref, stat_ref) = refs
        unpack_lines(g_ref, stat_ref)
    else:
        (k_ref, v_ref, kt_ref, tile_ref, chunk_ref, dk_in, dv_in, tab_in, q_ref, g_ref,
         stat_ref, _, dk_ref, dv_ref, out_tab_ref, dq_ref) = refs
    rows = k_ref.shape[0]
    size = tile_ref.shape[2]
    head_dim = k_ref.shape[1] // head_count
    inv_root = head_dim ** (-0.5)
    g_shift = -first_head * head_dim
    last_lines = []

    def one_head(local_head):
        head = local_head + first_head
        at = head * head_dim
        if not isinstance(local_head, int):
            at = pl.multiple_of(at, head_dim)
        cols = pl.ds(at, head_dim)
        key, value = k_ref[:, cols], v_ref[:, cols]
        query = q_ref[:, cols]
        grad = g_ref[:rows, pl.ds(at + g_shift, head_dim)]
        log_row = stat_ref[pl.ds(head, 1), :]
        dot_row = stat_ref[pl.ds(head + head_count, 1), :]
        const = chunk_ref[pl.ds(head, 1), :][:, 3 * size :]
        tiles = [None if lag == 2 else tile_ref[head, b] for b in range(3)]
        weights, scores, acc = score_terms(
            lag, key, value, query, grad, log_row, dot_row, tiles, const, inv_root
        )
        if lag == 0:
            turned = key.T
            kt_ref[cols, :] = turned
        else:
            turned = kt_ref[cols, :]
        dq = lax.dot_general(turned, scores, NN, preferred_element_type=F32) * inv_root
        dq_ref[cols, :] = dq.astype(dq_ref.dtype)
        lines = [
            jnp.zeros((1, size), F32) if line is None else line for line in table_lines(acc, size)
        ]
        lines = jnp.concatenate(lines, axis=1)
        if lag > 0:
            lines = tab_in[pl.ds(head, 1), :] + lines
        dk = lax.dot_general(scores, query, NN, preferred_element_type=F32)
        dv = lax.dot_general(weights, grad, NN, preferred_element_type=F32)
        if lag > 0:
            dk = dk + dk_in[:, cols]
            dv = dv + dv_in[:, cols]
        dk_ref[:, cols] = dk
        dv_ref[:, cols] = dv
        if first_head == 0:
            tab_ref[pl.ds(head, 1), :] = lines
        else:
            last_lines.append(lines)

    if first_head == 0:

        @pl.loop(0, (last_head - first_head) // heads_step)
        def _(step):
            for i in range(heads_step):
                one_head(step * heads_step + i)

    else:
        for i in range(last_head - first_head):
            one_head(i)
        table = jnp.concatenate([tab_in[:first_head, :]] + last_lines, axis=0)
        out_tab_ref[...] = fold_table(table, out_tab_ref.shape[1], size)


def close_kernel(heads_step, head_count, dq_ref, one_ref, two_ref, dk_ref, dv_ref,
                 gq_hbm, gk_hbm, gv_hbm, gq_ref, gk_ref, gv_ref, sems):
    head_dim = dq_ref.shape[0] // head_count
    inv_root = head_dim ** (-0.5)
    gk_ref[...] = (dk_ref[...] * inv_root).astype(BF16)
    copies = [pltpu.make_async_copy(gk_ref, gk_hbm, sems.at[0])]
    copies[-1].start()
    gv_ref[...] = dv_ref[...].astype(BF16)
    copies.append(pltpu.make_async_copy(gv_ref, gv_hbm, sems.at[1]))
    copies[-1].start()

    @pl.loop(0, head_count // heads_step)
    def _(step):
        for i in range(heads_step):
            cols = pl.ds(pl.multiple_of((step * heads_step + i) * head_dim, head_dim), head_dim)
            total = dq_ref[cols, :] + one_ref[cols, :].astype(F32) + two_ref[cols, :].astype(F32)
            gq_ref[:, cols] = total.T.astype(BF16)

    copies.append(pltpu.make_async_copy(gq_ref, gq_hbm, sems.at[2]))
    copies[-1].start()
    for copy in copies:
        copy.wait()


def local(query_rows, key_rows, value_rows, out_grad, log_totals, out_dot, bias_table):
    rows, feats = query_rows.shape
    heads = log_totals.shape[1]
    table_len = bias_table.shape[1]
    half = rows // 2
    cut_head = heads * 3 // 4
    head_dim = feats // heads
    cut = cut_head * head_dim
    vmem = pl.BlockSpec(memory_space=pltpu.VMEM)
    hbm = pl.BlockSpec(memory_space=pltpu.HBM)
    pair_flops = 2 * rows * rows * head_dim

    def call(body, work, outs, args, scratch=(), specs=None, out_specs=None, aliases={}):
        estimate = pl.CostEstimate(
            flops=int(work * pair_flops), bytes_accessed=8 * rows * feats, transcendentals=0
        )
        return pl.pallas_call(
            body,
            in_specs=[vmem] * len(args) if specs is None else specs,
            out_specs=[vmem] * len(outs) if out_specs is None else out_specs,
            out_shape=outs,
            scratch_shapes=list(scratch),
            input_output_aliases=aliases,
            cost_estimate=estimate,
            compiler_params=pltpu.CompilerParams(vmem_limit_bytes=16 * 2**20),
        )(*args)

    rows_f32 = pltpu.VMEM((rows, feats), F32)
    rows_b16 = pltpu.VMEM((rows, feats), BF16)
    turn_f32 = pltpu.VMEM((feats, rows), F32)
    turn_b16 = pltpu.VMEM((feats, rows), BF16)
    wide_tab = pltpu.VMEM((heads, 4 * half), F32)
    table_shape = pltpu.VMEM((heads, table_len), F32)
    tile_shape = pltpu.VMEM((heads, 3, half, half), F32)
    stat_shape = pltpu.VMEM((2 * heads, rows), F32)
    line_shape = pltpu.VMEM((heads, rows), F32)
    out_shape = jax.ShapeDtypeStruct((rows, feats), BF16)
    body = functools.partial

    def at_hbm(array):
        return pltpu.with_memory_space_constraint(array, pltpu.HBM)

    def packed_shape(height, width):
        return pltpu.VMEM((height + pack_height(2 * heads, rows, width), width), BF16)

    query_far = shifted(query_rows, -2)
    query_in = shifted(query_rows, -1)
    far, first, second, stats = call(
        prep_kernel, 1,
        [packed_shape(rows, feats), packed_shape(rows, cut),
         pltpu.VMEM((rows, feats - cut), BF16), stat_shape],
        tuple(at_hbm(x) for x in (out_grad, log_totals.T, out_dot.T)),
        (line_shape, line_shape, pltpu.SemaphoreType.DMA((5,))),
        [hbm] * 3,
    )
    far_in = shifted(far, -2)
    first_in = shifted(first, -1)
    second_in = shifted(second, -1)

    dq0, dk, dv, tab, turned, tiles, chunks, keys, values = call(
        body(lag_kernel, 0, 0, heads, 2, heads), 5 * heads,
        [turn_f32, rows_f32, rows_f32, wide_tab, turn_b16, tile_shape, wide_tab,
         rows_b16, rows_b16],
        tuple(at_hbm(x) for x in (key_rows, value_rows, query_rows, bias_table))
        + (far, stats),
        (rows_b16, table_shape, pltpu.SemaphoreType.DMA((4,))),
        [hbm] * 4 + [vmem] * 2,
    )
    shared = (keys, values, turned, tiles, chunks)
    dk, dv, tab, dq2, _ = call(
        body(lag_kernel, 2, 0, heads, 2, heads), 5 * heads,
        [rows_f32, rows_f32, wide_tab, turn_b16, stat_shape],
        shared + (dk, dv, tab, query_far, far_in), aliases={5: 0, 6: 1, 7: 2},
    )
    back_far = shifted(dq2, 2)
    dk, dv, tab, dq1, stats_in = call(
        body(lag_kernel, 1, 0, cut_head, 2, heads), 5 * cut_head,
        [rows_f32, rows_f32, wide_tab, turn_b16, stat_shape],
        shared + (dk, dv, tab) + (query_in, first_in), aliases={5: 0, 6: 1, 7: 2},
    )
    dk, dv, table_part, dq1 = call(
        body(lag_kernel, 1, cut_head, heads, 2, heads), 5 * (heads - cut_head),
        [rows_f32, rows_f32, table_shape, turn_b16],
        shared + (dk, dv, tab) + (query_in, second_in, stats_in, dq1),
        aliases={5: 0, 6: 1, 11: 3},
    )
    back_near = shifted(dq1, 1)
    grad_table = all_sum(table_part)
    grad_query, grad_key, grad_value = call(
        body(close_kernel, 2, heads), 1, [out_shape] * 3,
        (dq0, back_near, back_far, dk, dv),
        (rows_b16,) * 3 + (pltpu.SemaphoreType.DMA((3,)),),
        out_specs=[hbm] * 3,
    )
    return grad_query, grad_key, grad_value, grad_table


def solution(mesh):
    placed = (P(AXES, None),) * 6 + (P(),)
    return jax.shard_map(
        local,
        mesh=mesh,
        in_specs=placed,
        out_specs=(P(AXES, None),) * 3 + (P(),),
        check_vma=False,
    )
```

```python
import functools
import math

import jax
import jax.numpy as jnp
from jax import lax
from jax.experimental import pallas as pl
from jax.experimental.pallas import tpu as pltpu
from jax.sharding import PartitionSpec as P


SEG_LEN = 64
AXES = ("sp", "tp")
LOG2E = math.log2(math.e)
MASKED = -1e30
TERMS = 3
ROUND_ORDER = ((0,), (3, 4), (1, 2))
F32 = jnp.float32
BF16 = jnp.bfloat16
NT = (((1,), (1,)), ((), ()))
NN = (((1,), (0,)), ((), ()))


def shifted(block, distance):
    count = lax.axis_size(AXES)
    route = [(i - distance, i) for i in range(count) if 0 <= i - distance < count]
    return lax.ppermute(block, AXES, route)


def pair_tree(parts):
    while len(parts) > 1:
        parts = [parts[i] + parts[i + 1] for i in range(0, len(parts), 2)]
    return parts[0]


def table_rounds(count):
    twos = []
    stride = 1
    while count % (2 * stride) == 0:
        twos.append(stride)
        stride *= 2
    order = ROUND_ORDER
    rounds = [tuple(twos[d] for d in digits if d < len(twos)) for digits in order]
    used = sum(len(digits) for digits in order)
    rounds += [(twos[d],) for d in range(used, len(twos))]
    odd = []
    rest, factor = count // stride, 3
    while rest > 1:
        while rest % factor == 0:
            odd.append((stride, factor))
            stride *= factor
            rest //= factor
        factor += 2
    return [r for r in rounds if r], odd


def all_sum(part):
    count = lax.axis_size(AXES)
    me = lax.axis_index(AXES)
    binary, odd = table_rounds(count)
    for strides in binary:
        masks = [0]
        for stride in strides:
            masks += [mask ^ stride for mask in masks]
        parts = [part]
        for mask in masks[1:]:
            parts.append(lax.ppermute(part, AXES, [(i, i ^ mask) for i in range(count)]))
        part = pair_tree(parts)
    for stride, radix in odd:
        digit = (me // stride) % radix
        parts = [part]
        for step in range(1, radix):
            route = []
            for i in range(count):
                d = (i // stride) % radix
                route.append((i, i + (((d - step) % radix) - d) * stride))
            parts.append(lax.ppermute(part, AXES, route))
        total = jnp.zeros_like(part)
        for d in range(radix):
            value = parts[0]
            for step in range(1, radix):
                value = jnp.where((digit + step) % radix == d, parts[step], value)
            total = total + value
        part = total
    return part


def prep_tiles(head_count, table_ref, chunk_ref, tile_ref):
    size = tile_ref.shape[2]
    table_len = table_ref.shape[1]
    span = chunk_ref.shape[1]
    pad = size - (SEG_LEN - 1)
    lane = lax.broadcasted_iota(jnp.int32, (head_count, span), 1)
    table = table_ref[...] * LOG2E
    first, last = table[:, :1], table[:, table_len - 1 :]
    wide = jnp.concatenate([table, jnp.zeros((head_count, span - table_len), F32)], axis=1)
    moved = pltpu.roll(wide, pad, 1)
    moved = jnp.where(lane < pad, first, jnp.where(lane >= pad + table_len, last, moved))
    chunk_ref[...] = moved
    row = lax.broadcasted_iota(jnp.int32, (size, size), 0)
    col = lax.broadcasted_iota(jnp.int32, (size, size), 1)

    @pl.loop(0, head_count)
    def _(head):
        rolled = []
        lines = chunk_ref[pl.ds(head, 1), :]
        for c in range(4):
            line = jnp.broadcast_to(lines[:, c * size : (c + 1) * size], (size, size))
            rolled.append(pltpu.roll(line, 0, 1, stride=1, stride_axis=0))
        for b in range(3):
            tile = jnp.where(col >= row, rolled[b + 1], rolled[b])
            if b == 0:
                tile = jnp.where((row // SEG_LEN) <= (col // SEG_LEN), tile, MASKED)
            tile_ref[head, b] = tile


def unroll_sum(tile):
    size = tile.shape[0]
    group = 8
    parts = []
    for start in range(0, size, group):
        part = tile[start : start + group, :]
        parts.append(part if start == 0 else pltpu.roll(part, size - start, 1))
    total = pair_tree(parts)
    row = lax.broadcasted_iota(jnp.int32, total.shape, 0)
    for bit in (1, 2, 4):
        total = jnp.where((row & bit) != 0, pltpu.roll(total, size - bit, 1), total)
    return jnp.sum(total, axis=0, keepdims=True)


def score_terms(lag, raw_ref, wgt_ref, w_ref, s_ref, log_row, dot_row, tiles, const, inv_root):
    half = raw_ref.shape[0] // 2
    row = lax.broadcasted_iota(jnp.int32, (half, half), 0) // SEG_LEN
    col = lax.broadcasted_iota(jnp.int32, (half, half), 1) // SEG_LEN
    acc = [None, None, None, None]
    for r in range(2):
        for c in range(2):
            rs, cs = slice(r * half, (r + 1) * half), slice(c * half, (c + 1) * half)
            if (lag == 0 and r > c) or (lag == 2 and c > r):
                w_ref[rs, cs] = jnp.zeros((half, half), BF16)
                s_ref[rs, cs] = jnp.zeros((half, half), BF16)
                continue
            level = min(2 * lag + c - r, 3)
            lrow = log_row[:, cs]
            bias = const - lrow if level == 3 else tiles[level] - lrow
            weight = jnp.exp2(raw_ref[rs, cs] * (inv_root * LOG2E) + bias)
            if lag == 2 and r == c:
                weight = jnp.where(col <= row, weight, 0.0)
            score = weight * (wgt_ref[rs, cs] - dot_row[:, cs])
            acc[level] = score if acc[level] is None else acc[level] + score
            w_ref[rs, cs] = weight.astype(BF16)
            s_ref[rs, cs] = score.astype(BF16)
    return acc


def table_lines(acc, size):
    row = lax.broadcasted_iota(jnp.int32, (size, size), 0)
    col = lax.broadcasted_iota(jnp.int32, (size, size), 1)
    zero = jnp.zeros((size, size), F32)
    lines = []
    for c in range(4):
        upper = acc[c - 1] if c > 0 else None
        lower = acc[c] if c < 3 else None
        line = None
        if upper is not None or lower is not None:
            mixed = jnp.where(
                col >= row,
                zero if upper is None else upper,
                zero if lower is None else lower,
            )
            line = unroll_sum(mixed)
        if c == 3 and acc[3] is not None:
            extra = jnp.sum(acc[3], axis=0, keepdims=True)
            line = extra if line is None else line + extra
        lines.append(line)
    return lines


def fold_table(lines, table_len, size):
    pad = size - (SEG_LEN - 1)
    lane = lax.broadcasted_iota(jnp.int32, lines.shape, 1)
    tail = jnp.sum(jnp.where(lane >= pad + table_len - 1, lines, 0.0), axis=1, keepdims=True)
    moved = pltpu.roll(lines, lines.shape[1] - pad, 1)[:, :table_len]
    lane = lax.broadcasted_iota(jnp.int32, moved.shape, 1)
    return jnp.where(lane == table_len - 1, tail, moved)


def pack_height(count, rows, width):
    lines = -(-count * TERMS * rows // width)
    return -(-lines // 8) * 8


def pack_lines(stats, width):
    count, rows = stats.shape
    high = stats.astype(BF16).astype(F32)
    rest = stats - high
    mid = rest.astype(BF16).astype(F32)
    terms = (high, mid, rest - mid)
    per_row = width // rows
    lines = []
    for line in range(pack_height(count, rows, width)):
        pieces = []
        for b in range(line * per_row, (line + 1) * per_row):
            if b < count * TERMS:
                pieces.append(terms[b // count][b % count : b % count + 1, :])
            else:
                pieces.append(jnp.zeros((1, rows), F32))
        lines.append(jnp.concatenate(pieces, axis=1))
    return jnp.concatenate(lines, axis=0).astype(BF16)


def unpack_lines(pack_ref, stat_ref):
    count, rows = stat_ref.shape
    per_row = pack_ref.shape[1] // rows
    packed = pack_ref[rows:, :].astype(F32)
    for i in range(count):
        total = None
        for term in range(TERMS):
            line, at = divmod(term * count + i, per_row)
            piece = packed[line : line + 1, at * rows : (at + 1) * rows]
            total = piece if total is None else total + piece
        stat_ref[i : i + 1, :] = total


def prep_kernel(g_hbm, log_hbm, dot_hbm, far_ref, first_ref, second_ref, stat_ref,
                log_ref, dot_ref, sems):
    rows, feats = g_hbm.shape
    cut = first_ref.shape[1]
    moves = (
        (log_hbm, log_ref),
        (dot_hbm, dot_ref),
        (g_hbm, far_ref.at[pl.ds(0, rows), :]),
        (g_hbm.at[:, pl.ds(0, cut)], first_ref.at[pl.ds(0, rows), :]),
        (g_hbm.at[:, pl.ds(cut, feats - cut)], second_ref),
    )
    copies = []
    for i, (origin, target) in enumerate(moves):
        copies.append(pltpu.make_async_copy(origin, target, sems.at[i]))
        copies[-1].start()
    for copy in copies[:2]:
        copy.wait()
    stats = jnp.concatenate([log_ref[...] * LOG2E, dot_ref[...]], axis=0)
    stat_ref[...] = stats
    first_ref[rows:, :] = pack_lines(stats, first_ref.shape[1])
    far_ref[rows:, :] = pack_lines(stats, far_ref.shape[1])
    for copy in copies[2:]:
        copy.wait()


def lag_kernel(lag, first_head, last_head, head_count, *refs):
    raw_refs, wgt_refs, w_refs, s_refs = (refs[len(refs) - 8 + 2 * i :][:2] for i in range(4))
    refs = refs[:-8]
    if lag == 0:
        (k_hbm, v_hbm, q_hbm, table_hbm, g_ref, stat_ref,
         dq_ref, dk_ref, dv_ref, tab_ref, kt_ref, tile_ref, chunk_ref, k_ref, v_ref,
         q_ref, table_ref, sems) = refs
        pairs = ((table_hbm, table_ref), (k_hbm, k_ref), (v_hbm, v_ref), (q_hbm, q_ref))
        copies = []
        for i, (source, target) in enumerate(pairs):
            copies.append(pltpu.make_async_copy(source, target, sems.at[i]))
            copies[-1].start()
        copies[0].wait()
        prep_tiles(head_count, table_ref, chunk_ref, tile_ref)
        for copy in copies[1:]:
            copy.wait()
    elif lag == 2:
        (k_ref, v_ref, kt_ref, tile_ref, chunk_ref, dk_in, dv_in, tab_in, q_ref, g_ref,
         dk_ref, dv_ref, tab_ref, dq_ref, stat_ref) = refs
        unpack_lines(g_ref, stat_ref)
    elif first_head == 0:
        (k_ref, v_ref, kt_ref, tile_ref, chunk_ref, dk_in, dv_in, tab_in, q_ref, g_ref,
         dk_ref, dv_ref, tab_ref, dq_ref, stat_ref) = refs
        unpack_lines(g_ref, stat_ref)
    else:
        (k_ref, v_ref, kt_ref, tile_ref, chunk_ref, dk_in, dv_in, tab_in, q_ref, g_ref,
         stat_ref, _, dk_ref, dv_ref, out_tab_ref, dq_ref) = refs
    rows = k_ref.shape[0]
    size = tile_ref.shape[2]
    head_dim = k_ref.shape[1] // head_count
    inv_root = head_dim ** (-0.5)
    g_shift = -first_head * head_dim
    last_lines = []

    def span(head):
        return slice(head * head_dim, (head + 1) * head_dim)

    def products(head, at):
        local = slice(head * head_dim + g_shift, (head + 1) * head_dim + g_shift)
        query, grad = q_ref[:, span(head)], g_ref[:rows, local]
        raw_refs[at][...] = lax.dot_general(
            k_ref[:, span(head)], query, NT, preferred_element_type=F32
        )
        wgt_refs[at][...] = lax.dot_general(
            v_ref[:, span(head)], grad, NT, preferred_element_type=F32
        )

    def scores(head, at):
        log_row = stat_ref[head : head + 1, :]
        dot_row = stat_ref[head + head_count : head + head_count + 1, :]
        const = chunk_ref[head : head + 1, 3 * size :]
        tiles = [None if lag == 2 else tile_ref[head, b] for b in range(3)]
        acc = score_terms(
            lag, raw_refs[at], wgt_refs[at], w_refs[at], s_refs[at],
            log_row, dot_row, tiles, const, inv_root,
        )
        lines = [
            jnp.zeros((1, size), F32) if line is None else line for line in table_lines(acc, size)
        ]
        lines = jnp.concatenate(lines, axis=1)
        if lag > 0:
            lines = tab_in[head : head + 1, :] + lines
        if first_head == 0:
            tab_ref[head : head + 1, :] = lines
        else:
            last_lines.append(lines)

    def gradients(head, at):
        cols = span(head)
        local = slice(head * head_dim + g_shift, (head + 1) * head_dim + g_shift)
        if lag == 0:
            turned = k_ref[:, cols].T
            kt_ref[cols, :] = turned
        else:
            turned = kt_ref[cols, :]
        score_b = s_refs[at][...]
        dq = lax.dot_general(turned, score_b, NN, preferred_element_type=F32) * inv_root
        dq_ref[cols, :] = dq.astype(dq_ref.dtype)
        dk = lax.dot_general(score_b, q_ref[:, cols], NN, preferred_element_type=F32)
        dv = lax.dot_general(w_refs[at][...], g_ref[:rows, local], NN, preferred_element_type=F32)
        if lag > 0:
            dk = dk + dk_in[:, cols]
            dv = dv + dv_in[:, cols]
        dk_ref[:, cols] = dk
        dv_ref[:, cols] = dv

    stages = (products, scores, gradients)
    steps = last_head - first_head + len(stages) - 1
    for step in range(steps):
        for depth, stage in enumerate(stages):
            head = first_head + step - depth
            if first_head <= head < last_head:
                stage(head, head % 2)

    if first_head > 0:
        table = jnp.concatenate([tab_in[:first_head, :]] + last_lines, axis=0)
        out_tab_ref[...] = fold_table(table, out_tab_ref.shape[1], size)


def key_value_kernel(scale, dk_ref, dv_ref, gk_hbm, gv_hbm, gk_ref, gv_ref, sems):
    gk_ref[...] = (dk_ref[...] * scale).astype(BF16)
    copies = [pltpu.make_async_copy(gk_ref, gk_hbm, sems.at[0])]
    copies[0].start()
    gv_ref[...] = dv_ref[...].astype(BF16)
    copies.append(pltpu.make_async_copy(gv_ref, gv_hbm, sems.at[1]))
    copies[1].start()
    for copy in copies:
        copy.wait()


def query_kernel(head_count, dq_ref, one_ref, two_ref, gq_hbm, gq_ref, sems):
    head_dim = dq_ref.shape[0] // head_count
    copies = []
    for head in range(head_count):
        cols = slice(head * head_dim, (head + 1) * head_dim)
        total = dq_ref[cols, :] + one_ref[cols, :].astype(F32) + two_ref[cols, :].astype(F32)
        gq_ref[:, cols] = total.T.astype(BF16)
        if head % 4 == 3:
            part = pl.ds((head - 3) * head_dim, 4 * head_dim)
            copies.append(
                pltpu.make_async_copy(gq_ref.at[:, part], gq_hbm.at[:, part], sems.at[head // 4])
            )
            copies[-1].start()
    for copy in copies:
        copy.wait()


def local(query_rows, key_rows, value_rows, out_grad, log_totals, out_dot, bias_table):
    rows, feats = query_rows.shape
    heads = log_totals.shape[1]
    table_len = bias_table.shape[1]
    half = rows // 2
    cut_head = heads * 3 // 4
    head_dim = feats // heads
    cut = cut_head * head_dim
    vmem = pl.BlockSpec(memory_space=pltpu.VMEM)
    hbm = pl.BlockSpec(memory_space=pltpu.HBM)
    pair_flops = 2 * rows * rows * head_dim

    def call(body, work, outs, args, scratch=(), specs=None, out_specs=None, aliases={}):
        estimate = pl.CostEstimate(
            flops=int(work * pair_flops), bytes_accessed=8 * rows * feats, transcendentals=0
        )
        return pl.pallas_call(
            body,
            in_specs=[vmem] * len(args) if specs is None else specs,
            out_specs=[vmem] * len(outs) if out_specs is None else out_specs,
            out_shape=outs,
            scratch_shapes=list(scratch),
            input_output_aliases=aliases,
            cost_estimate=estimate,
            compiler_params=pltpu.CompilerParams(vmem_limit_bytes=16 * 2**20),
        )(*args)

    rows_f32 = pltpu.VMEM((rows, feats), F32)
    rows_b16 = pltpu.VMEM((rows, feats), BF16)
    turn_f32 = pltpu.VMEM((feats, rows), F32)
    turn_b16 = pltpu.VMEM((feats, rows), BF16)
    wide_tab = pltpu.VMEM((heads, 4 * half), F32)
    table_shape = pltpu.VMEM((heads, table_len), F32)
    tile_shape = pltpu.VMEM((heads, 3, half, half), F32)
    stat_shape = pltpu.VMEM((2 * heads, rows), F32)
    line_shape = pltpu.VMEM((heads, rows), F32)
    out_shape = jax.ShapeDtypeStruct((rows, feats), BF16)
    stage_shapes = (pltpu.VMEM((rows, rows), F32),) * 4 + (pltpu.VMEM((rows, rows), BF16),) * 4
    body = functools.partial

    def at_hbm(array):
        return pltpu.with_memory_space_constraint(array, pltpu.HBM)

    def packed_shape(height, width):
        return pltpu.VMEM((height + pack_height(2 * heads, rows, width), width), BF16)

    query_far = shifted(query_rows, -2)
    query_in = shifted(query_rows, -1)
    far, first, second, stats = call(
        prep_kernel, 1,
        [packed_shape(rows, feats), packed_shape(rows, cut),
         pltpu.VMEM((rows, feats - cut), BF16), stat_shape],
        tuple(at_hbm(x) for x in (out_grad, log_totals.T, out_dot.T)),
        (line_shape, line_shape, pltpu.SemaphoreType.DMA((5,))),
        [hbm] * 3,
    )
    far_in = shifted(far, -2)
    first_in = shifted(first, -1)
    second_in = shifted(second, -1)

    dq0, dk, dv, tab, turned, tiles, chunks, keys, values = call(
        body(lag_kernel, 0, 0, heads, heads), 5 * heads,
        [turn_f32, rows_f32, rows_f32, wide_tab, turn_b16, tile_shape, wide_tab,
         rows_b16, rows_b16],
        tuple(at_hbm(x) for x in (key_rows, value_rows, query_rows, bias_table))
        + (far, stats),
        (rows_b16, table_shape, pltpu.SemaphoreType.DMA((4,))) + stage_shapes,
        [hbm] * 4 + [vmem] * 2,
    )
    shared = (keys, values, turned, tiles, chunks)
    dk, dv, tab, dq2, _ = call(
        body(lag_kernel, 2, 0, heads, heads), 5 * heads,
        [rows_f32, rows_f32, wide_tab, turn_b16, stat_shape],
        shared + (dk, dv, tab, query_far, far_in), stage_shapes, aliases={5: 0, 6: 1, 7: 2},
    )
    back_far = shifted(dq2, 2)
    dk, dv, tab, dq1, stats_in = call(
        body(lag_kernel, 1, 0, cut_head, heads), 5 * cut_head,
        [rows_f32, rows_f32, wide_tab, turn_b16, stat_shape],
        shared + (dk, dv, tab) + (query_in, first_in), stage_shapes, aliases={5: 0, 6: 1, 7: 2},
    )
    dk, dv, table_part, dq1 = call(
        body(lag_kernel, 1, cut_head, heads, heads), 5 * (heads - cut_head),
        [rows_f32, rows_f32, table_shape, turn_b16],
        shared + (dk, dv, tab) + (query_in, second_in, stats_in, dq1), stage_shapes,
        aliases={5: 0, 6: 1, 11: 3},
    )
    back_near = shifted(dq1, 1)
    grad_table = all_sum(table_part)
    grad_key, grad_value = call(
        body(key_value_kernel, head_dim ** (-0.5)), 1, [out_shape] * 2, (dk, dv),
        (rows_b16,) * 2 + (pltpu.SemaphoreType.DMA((2,)),), out_specs=[hbm] * 2,
    )
    grad_query, = call(
        body(query_kernel, heads), 1, [out_shape], (dq0, back_near, back_far),
        (rows_b16, pltpu.SemaphoreType.DMA((heads // 4,))), out_specs=[hbm],
    )
    return grad_query, grad_key, grad_value, grad_table


def solution(mesh):
    placed = (P(AXES, None),) * 6 + (P(),)
    return jax.shard_map(
        local,
        mesh=mesh,
        in_specs=placed,
        out_specs=(P(AXES, None),) * 3 + (P(),),
        check_vma=False,
    )
```

```python
import functools
import math

import jax
import jax.numpy as jnp
from jax import lax
from jax.experimental import pallas as pl
from jax.experimental.pallas import tpu as pltpu
from jax.sharding import PartitionSpec as P


SEG_LEN = 64
AXES = ("sp", "tp")
LOG2E = math.log2(math.e)
MASKED = -1e30
TERMS = 3
ROUND_ORDER = ((0,), (3, 4), (1, 2))
F32 = jnp.float32
BF16 = jnp.bfloat16
NT = (((1,), (1,)), ((), ()))
NN = (((1,), (0,)), ((), ()))


def shifted(block, distance):
    count = lax.axis_size(AXES)
    route = [(i - distance, i) for i in range(count) if 0 <= i - distance < count]
    return lax.ppermute(block, AXES, route)


def pair_tree(parts):
    while len(parts) > 1:
        parts = [parts[i] + parts[i + 1] for i in range(0, len(parts), 2)]
    return parts[0]


def table_rounds(count):
    twos = []
    stride = 1
    while count % (2 * stride) == 0:
        twos.append(stride)
        stride *= 2
    order = ROUND_ORDER
    rounds = [tuple(twos[d] for d in digits if d < len(twos)) for digits in order]
    used = sum(len(digits) for digits in order)
    rounds += [(twos[d],) for d in range(used, len(twos))]
    odd = []
    rest, factor = count // stride, 3
    while rest > 1:
        while rest % factor == 0:
            odd.append((stride, factor))
            stride *= factor
            rest //= factor
        factor += 2
    return [r for r in rounds if r], odd


def all_sum(part):
    count = lax.axis_size(AXES)
    me = lax.axis_index(AXES)
    binary, odd = table_rounds(count)
    at = 0
    for strides in binary:
        masks = [0]
        for stride in strides:
            masks += [mask ^ stride for mask in masks]
        parts = [part]
        for mask in masks[1:]:
            parts.append(lax.ppermute(part, AXES, [(i, i ^ mask) for i in range(count)]))
        if at == len(binary) - 1 and not odd:
            return parts
        part = pair_tree(parts)
        at += 1
    for stride, radix in odd:
        digit = (me // stride) % radix
        parts = [part]
        for step in range(1, radix):
            route = []
            for i in range(count):
                d = (i // stride) % radix
                route.append((i, i + (((d - step) % radix) - d) * stride))
            parts.append(lax.ppermute(part, AXES, route))
        total = jnp.zeros_like(part)
        for d in range(radix):
            value = parts[0]
            for step in range(1, radix):
                value = jnp.where((digit + step) % radix == d, parts[step], value)
            total = total + value
        part = total
        at += 1
    return [part]


def prep_tiles(head_count, table_ref, chunk_ref, tile_ref):
    size = tile_ref.shape[2]
    table_len = table_ref.shape[1]
    span = chunk_ref.shape[1]
    pad = size - (SEG_LEN - 1)
    lane = lax.broadcasted_iota(jnp.int32, (head_count, span), 1)
    table = table_ref[...] * LOG2E
    first, last = table[:, :1], table[:, table_len - 1 :]
    wide = jnp.concatenate([table, jnp.zeros((head_count, span - table_len), F32)], axis=1)
    moved = pltpu.roll(wide, pad, 1)
    moved = jnp.where(lane < pad, first, jnp.where(lane >= pad + table_len, last, moved))
    chunk_ref[...] = moved
    row = lax.broadcasted_iota(jnp.int32, (size, size), 0)
    col = lax.broadcasted_iota(jnp.int32, (size, size), 1)

    @pl.loop(0, head_count)
    def _(head):
        rolled = []
        lines = chunk_ref[pl.ds(head, 1), :]
        for c in range(4):
            line = jnp.broadcast_to(lines[:, c * size : (c + 1) * size], (size, size))
            rolled.append(pltpu.roll(line, 0, 1, stride=1, stride_axis=0))
        for b in range(3):
            tile = jnp.where(col >= row, rolled[b + 1], rolled[b])
            if b == 0:
                tile = jnp.where((row // SEG_LEN) <= (col // SEG_LEN), tile, MASKED)
            tile_ref[head, b] = tile


def unroll_sum(tile):
    size = tile.shape[0]
    group = 8
    parts = []
    for start in range(0, size, group):
        part = tile[start : start + group, :]
        parts.append(part if start == 0 else pltpu.roll(part, size - start, 1))
    total = pair_tree(parts)
    row = lax.broadcasted_iota(jnp.int32, total.shape, 0)
    for bit in (1, 2, 4):
        total = jnp.where((row & bit) != 0, pltpu.roll(total, size - bit, 1), total)
    return jnp.sum(total, axis=0, keepdims=True)


def score_terms(lag, raw_ref, wgt_ref, w_ref, s_ref, log_row, dot_row, tiles, const, inv_root):
    half = raw_ref.shape[0] // 2
    row = lax.broadcasted_iota(jnp.int32, (half, half), 0) // SEG_LEN
    col = lax.broadcasted_iota(jnp.int32, (half, half), 1) // SEG_LEN
    acc = [None, None, None, None]
    for r in range(2):
        for c in range(2):
            rs, cs = slice(r * half, (r + 1) * half), slice(c * half, (c + 1) * half)
            if (lag == 0 and r > c) or (lag == 2 and c > r):
                w_ref[rs, cs] = jnp.zeros((half, half), BF16)
                s_ref[rs, cs] = jnp.zeros((half, half), BF16)
                continue
            level = min(2 * lag + c - r, 3)
            lrow = log_row[:, cs]
            bias = const - lrow if level == 3 else tiles[level] - lrow
            weight = jnp.exp2(raw_ref[rs, cs] * (inv_root * LOG2E) + bias)
            if lag == 2 and r == c:
                weight = jnp.where(col <= row, weight, 0.0)
            score = weight * (wgt_ref[rs, cs] - dot_row[:, cs])
            acc[level] = score if acc[level] is None else acc[level] + score
            w_ref[rs, cs] = weight.astype(BF16)
            s_ref[rs, cs] = score.astype(BF16)
    return acc


def table_lines(acc, size):
    row = lax.broadcasted_iota(jnp.int32, (size, size), 0)
    col = lax.broadcasted_iota(jnp.int32, (size, size), 1)
    zero = jnp.zeros((size, size), F32)
    lines = []
    for c in range(4):
        upper = acc[c - 1] if c > 0 else None
        lower = acc[c] if c < 3 else None
        line = None
        if upper is not None or lower is not None:
            mixed = jnp.where(
                col >= row,
                zero if upper is None else upper,
                zero if lower is None else lower,
            )
            line = unroll_sum(mixed)
        if c == 3 and acc[3] is not None:
            extra = jnp.sum(acc[3], axis=0, keepdims=True)
            line = extra if line is None else line + extra
        lines.append(line)
    return lines


def fold_table(lines, table_len, size):
    pad = size - (SEG_LEN - 1)
    lane = lax.broadcasted_iota(jnp.int32, lines.shape, 1)
    tail = jnp.sum(jnp.where(lane >= pad + table_len - 1, lines, 0.0), axis=1, keepdims=True)
    moved = pltpu.roll(lines, lines.shape[1] - pad, 1)[:, :table_len]
    lane = lax.broadcasted_iota(jnp.int32, moved.shape, 1)
    return jnp.where(lane == table_len - 1, tail, moved)


def pack_height(count, rows, width):
    lines = -(-count * TERMS * rows // width)
    return -(-lines // 8) * 8


def pack_lines(stats, width):
    count, rows = stats.shape
    high = stats.astype(BF16).astype(F32)
    rest = stats - high
    mid = rest.astype(BF16).astype(F32)
    terms = (high, mid, rest - mid)
    per_row = width // rows
    lines = []
    for line in range(pack_height(count, rows, width)):
        pieces = []
        for b in range(line * per_row, (line + 1) * per_row):
            if b < count * TERMS:
                pieces.append(terms[b // count][b % count : b % count + 1, :])
            else:
                pieces.append(jnp.zeros((1, rows), F32))
        lines.append(jnp.concatenate(pieces, axis=1))
    return jnp.concatenate(lines, axis=0).astype(BF16)


def unpack_lines(pack_ref, stat_ref):
    count, rows = stat_ref.shape
    per_row = pack_ref.shape[1] // rows
    packed = pack_ref[rows:, :].astype(F32)
    for i in range(count):
        total = None
        for term in range(TERMS):
            line, at = divmod(term * count + i, per_row)
            piece = packed[line : line + 1, at * rows : (at + 1) * rows]
            total = piece if total is None else total + piece
        stat_ref[i : i + 1, :] = total


def prep_kernel(g_hbm, log_hbm, dot_hbm, far_ref, first_ref, second_ref, stat_ref,
                log_ref, dot_ref, sems):
    rows, feats = g_hbm.shape
    cut = first_ref.shape[1]
    moves = (
        (log_hbm, log_ref),
        (dot_hbm, dot_ref),
        (g_hbm, far_ref.at[pl.ds(0, rows), :]),
        (g_hbm.at[:, pl.ds(0, cut)], first_ref.at[pl.ds(0, rows), :]),
        (g_hbm.at[:, pl.ds(cut, feats - cut)], second_ref),
    )
    copies = []
    for i, (origin, target) in enumerate(moves):
        copies.append(pltpu.make_async_copy(origin, target, sems.at[i]))
        copies[-1].start()
    for copy in copies[:2]:
        copy.wait()
    stats = jnp.concatenate([log_ref[...] * LOG2E, dot_ref[...]], axis=0)
    stat_ref[...] = stats
    first_ref[rows:, :] = pack_lines(stats, first_ref.shape[1])
    far_ref[rows:, :] = pack_lines(stats, far_ref.shape[1])
    for copy in copies[2:]:
        copy.wait()


def lag_kernel(lag, first_head, last_head, head_count, *refs):
    raw_refs, wgt_refs, w_refs, s_refs = (refs[len(refs) - 8 + 2 * i :][:2] for i in range(4))
    refs = refs[:-8]
    if lag == 0:
        (k_hbm, v_hbm, q_hbm, table_hbm, g_ref, stat_ref,
         dq_ref, dk_ref, dv_ref, tab_ref, kt_ref, tile_ref, chunk_ref, k_ref, v_ref,
         q_ref, table_ref, sems) = refs
        pairs = ((table_hbm, table_ref), (k_hbm, k_ref), (v_hbm, v_ref), (q_hbm, q_ref))
        copies = []
        for i, (source, target) in enumerate(pairs):
            copies.append(pltpu.make_async_copy(source, target, sems.at[i]))
            copies[-1].start()
        copies[0].wait()
        prep_tiles(head_count, table_ref, chunk_ref, tile_ref)
        for copy in copies[1:]:
            copy.wait()
    elif lag == 2:
        (k_ref, v_ref, kt_ref, tile_ref, chunk_ref, dk_in, dv_in, tab_in, q_ref, g_ref,
         dk_ref, dv_ref, tab_ref, dq_ref, stat_ref) = refs
        unpack_lines(g_ref, stat_ref)
    elif first_head == 0:
        (k_ref, v_ref, kt_ref, tile_ref, chunk_ref, dk_in, dv_in, tab_in, q_ref, g_ref,
         dk_ref, dv_ref, tab_ref, dq_ref, stat_ref) = refs
        unpack_lines(g_ref, stat_ref)
    else:
        (k_ref, v_ref, kt_ref, tile_ref, chunk_ref, dk_in, dv_in, tab_in, q_ref, g_ref,
         stat_ref, _, dk_ref, dv_ref, out_tab_ref, dq_ref) = refs
    rows = k_ref.shape[0]
    size = tile_ref.shape[2]
    head_dim = k_ref.shape[1] // head_count
    inv_root = head_dim ** (-0.5)
    g_shift = -first_head * head_dim
    last_lines = []

    def span(head):
        return slice(head * head_dim, (head + 1) * head_dim)

    def products(head, at):
        local = slice(head * head_dim + g_shift, (head + 1) * head_dim + g_shift)
        query, grad = q_ref[:, span(head)], g_ref[:rows, local]
        raw_refs[at][...] = lax.dot_general(
            k_ref[:, span(head)], query, NT, preferred_element_type=F32
        )
        wgt_refs[at][...] = lax.dot_general(
            v_ref[:, span(head)], grad, NT, preferred_element_type=F32
        )

    def scores(head, at):
        log_row = stat_ref[head : head + 1, :]
        dot_row = stat_ref[head + head_count : head + head_count + 1, :]
        const = chunk_ref[head : head + 1, 3 * size :]
        tiles = [None if lag == 2 else tile_ref[head, b] for b in range(3)]
        acc = score_terms(
            lag, raw_refs[at], wgt_refs[at], w_refs[at], s_refs[at],
            log_row, dot_row, tiles, const, inv_root,
        )
        lines = [
            jnp.zeros((1, size), F32) if line is None else line for line in table_lines(acc, size)
        ]
        lines = jnp.concatenate(lines, axis=1)
        if lag > 0:
            lines = tab_in[head : head + 1, :] + lines
        if first_head == 0:
            tab_ref[head : head + 1, :] = lines
        else:
            last_lines.append(lines)

    def gradients(head, at):
        cols = span(head)
        local = slice(head * head_dim + g_shift, (head + 1) * head_dim + g_shift)
        if lag == 0:
            turned = k_ref[:, cols].T
            kt_ref[cols, :] = turned
        else:
            turned = kt_ref[cols, :]
        score_b = s_refs[at][...]
        dq = lax.dot_general(turned, score_b, NN, preferred_element_type=F32) * inv_root
        dq_ref[cols, :] = dq.astype(dq_ref.dtype)
        dk = lax.dot_general(score_b, q_ref[:, cols], NN, preferred_element_type=F32)
        dv = lax.dot_general(w_refs[at][...], g_ref[:rows, local], NN, preferred_element_type=F32)
        if lag > 0:
            dk = dk + dk_in[:, cols]
            dv = dv + dv_in[:, cols]
        dk_ref[:, cols] = dk
        dv_ref[:, cols] = dv

    stages = (products, scores, gradients)
    steps = last_head - first_head + len(stages) - 1
    for step in range(steps):
        for depth, stage in enumerate(stages):
            head = first_head + step - depth
            if first_head <= head < last_head:
                stage(head, head % 2)

    if first_head > 0:
        table = jnp.concatenate([tab_in[:first_head, :]] + last_lines, axis=0)
        out_tab_ref[...] = fold_table(table, out_tab_ref.shape[1], size)


def key_value_kernel(scale, dk_ref, dv_ref, gk_hbm, gv_hbm, gk_ref, gv_ref, sems):
    gk_ref[...] = (dk_ref[...] * scale).astype(BF16)
    copies = [pltpu.make_async_copy(gk_ref, gk_hbm, sems.at[0])]
    copies[0].start()
    gv_ref[...] = dv_ref[...].astype(BF16)
    copies.append(pltpu.make_async_copy(gv_ref, gv_hbm, sems.at[1]))
    copies[1].start()
    for copy in copies:
        copy.wait()


def query_kernel(head_count, dq_ref, one_ref, two_ref, *refs):
    term_refs = refs[:-5]
    gq_hbm, table_hbm, gq_ref, table_ref, sems = refs[-5:]
    table_ref[...] = pair_tree([ref[...] for ref in term_refs])
    head_dim = dq_ref.shape[0] // head_count
    copies = [pltpu.make_async_copy(table_ref, table_hbm, sems.at[0])]
    copies[0].start()
    for head in range(head_count):
        cols = slice(head * head_dim, (head + 1) * head_dim)
        total = dq_ref[cols, :] + one_ref[cols, :].astype(F32) + two_ref[cols, :].astype(F32)
        gq_ref[:, cols] = total.T.astype(BF16)
        if head % 4 == 3:
            part = pl.ds((head - 3) * head_dim, 4 * head_dim)
            copies.append(
                pltpu.make_async_copy(gq_ref.at[:, part], gq_hbm.at[:, part], sems.at[1 + head // 4])
            )
            copies[-1].start()
    for copy in copies:
        copy.wait()


def local(query_rows, key_rows, value_rows, out_grad, log_totals, out_dot, bias_table):
    rows, feats = query_rows.shape
    heads = log_totals.shape[1]
    table_len = bias_table.shape[1]
    half = rows // 2
    cut_head = heads * 3 // 4
    head_dim = feats // heads
    cut = cut_head * head_dim
    vmem = pl.BlockSpec(memory_space=pltpu.VMEM)
    hbm = pl.BlockSpec(memory_space=pltpu.HBM)
    pair_flops = 2 * rows * rows * head_dim

    def call(body, work, outs, args, scratch=(), specs=None, out_specs=None, aliases={}):
        estimate = pl.CostEstimate(
            flops=int(work * pair_flops), bytes_accessed=8 * rows * feats, transcendentals=0
        )
        return pl.pallas_call(
            body,
            in_specs=[vmem] * len(args) if specs is None else specs,
            out_specs=[vmem] * len(outs) if out_specs is None else out_specs,
            out_shape=outs,
            scratch_shapes=list(scratch),
            input_output_aliases=aliases,
            cost_estimate=estimate,
            compiler_params=pltpu.CompilerParams(vmem_limit_bytes=16 * 2**20),
        )(*args)

    rows_f32 = pltpu.VMEM((rows, feats), F32)
    rows_b16 = pltpu.VMEM((rows, feats), BF16)
    turn_f32 = pltpu.VMEM((feats, rows), F32)
    turn_b16 = pltpu.VMEM((feats, rows), BF16)
    wide_tab = pltpu.VMEM((heads, 4 * half), F32)
    table_shape = pltpu.VMEM((heads, table_len), F32)
    tile_shape = pltpu.VMEM((heads, 3, half, half), F32)
    stat_shape = pltpu.VMEM((2 * heads, rows), F32)
    line_shape = pltpu.VMEM((heads, rows), F32)
    out_shape = jax.ShapeDtypeStruct((rows, feats), BF16)
    stage_shapes = (pltpu.VMEM((rows, rows), F32),) * 4 + (pltpu.VMEM((rows, rows), BF16),) * 4
    body = functools.partial

    def at_hbm(array):
        return pltpu.with_memory_space_constraint(array, pltpu.HBM)

    def packed_shape(height, width):
        return pltpu.VMEM((height + pack_height(2 * heads, rows, width), width), BF16)

    query_far = shifted(query_rows, -2)
    query_in = shifted(query_rows, -1)
    far, first, second, stats = call(
        prep_kernel, 1,
        [packed_shape(rows, feats), packed_shape(rows, cut),
         pltpu.VMEM((rows, feats - cut), BF16), stat_shape],
        tuple(at_hbm(x) for x in (out_grad, log_totals.T, out_dot.T)),
        (line_shape, line_shape, pltpu.SemaphoreType.DMA((5,))),
        [hbm] * 3,
    )
    far_in = shifted(far, -2)
    first_in = shifted(first, -1)
    second_in = shifted(second, -1)

    dq0, dk, dv, tab, turned, tiles, chunks, keys, values = call(
        body(lag_kernel, 0, 0, heads, heads), 5 * heads,
        [turn_f32, rows_f32, rows_f32, wide_tab, turn_b16, tile_shape, wide_tab,
         rows_b16, rows_b16],
        tuple(at_hbm(x) for x in (key_rows, value_rows, query_rows, bias_table))
        + (far, stats),
        (rows_b16, table_shape, pltpu.SemaphoreType.DMA((4,))) + stage_shapes,
        [hbm] * 4 + [vmem] * 2,
    )
    shared = (keys, values, turned, tiles, chunks)
    dk, dv, tab, dq2, _ = call(
        body(lag_kernel, 2, 0, heads, heads), 5 * heads,
        [rows_f32, rows_f32, wide_tab, turn_b16, stat_shape],
        shared + (dk, dv, tab, query_far, far_in), stage_shapes, aliases={5: 0, 6: 1, 7: 2},
    )
    back_far = shifted(dq2, 2)
    dk, dv, tab, dq1, stats_in = call(
        body(lag_kernel, 1, 0, cut_head, heads), 5 * cut_head,
        [rows_f32, rows_f32, wide_tab, turn_b16, stat_shape],
        shared + (dk, dv, tab) + (query_in, first_in), stage_shapes, aliases={5: 0, 6: 1, 7: 2},
    )
    dk, dv, table_part, dq1 = call(
        body(lag_kernel, 1, cut_head, heads, heads), 5 * (heads - cut_head),
        [rows_f32, rows_f32, table_shape, turn_b16],
        shared + (dk, dv, tab) + (query_in, second_in, stats_in, dq1), stage_shapes,
        aliases={5: 0, 6: 1, 11: 3},
    )
    back_near = shifted(dq1, 1)
    table_terms = all_sum(table_part)
    grad_key, grad_value = call(
        body(key_value_kernel, head_dim ** (-0.5)), 1, [out_shape] * 2, (dk, dv),
        (rows_b16,) * 2 + (pltpu.SemaphoreType.DMA((2,)),), out_specs=[hbm] * 2,
    )
    table_out = jax.ShapeDtypeStruct((heads, table_len), F32)
    grad_query, grad_table = call(
        body(query_kernel, heads), 1, [out_shape, table_out],
        (dq0, back_near, back_far, *table_terms),
        (rows_b16, table_shape, pltpu.SemaphoreType.DMA((1 + heads // 4,))),
        out_specs=[hbm] * 2,
    )
    return grad_query, grad_key, grad_value, grad_table


def solution(mesh):
    placed = (P(AXES, None),) * 6 + (P(),)
    return jax.shard_map(
        local,
        mesh=mesh,
        in_specs=placed,
        out_specs=(P(AXES, None),) * 3 + (P(),),
        check_vma=False,
    )
```

```python
import functools
import math

import jax
import jax.numpy as jnp
from jax import lax
from jax.experimental import pallas as pl
from jax.experimental.pallas import tpu as pltpu
from jax.sharding import PartitionSpec as P


SEG_LEN = 64
AXES = ("sp", "tp")
LOG2E = math.log2(math.e)
MASKED = -1e30
TERMS = 3
ROUND_ORDER = ((0,), (3, 4), (1, 2))
F32 = jnp.float32
BF16 = jnp.bfloat16
NT = (((1,), (1,)), ((), ()))
NN = (((1,), (0,)), ((), ()))


def shifted(block, distance):
    count = lax.axis_size(AXES)
    route = [(i - distance, i) for i in range(count) if 0 <= i - distance < count]
    return lax.ppermute(block, AXES, route)


def pair_tree(parts):
    while len(parts) > 1:
        parts = [parts[i] + parts[i + 1] for i in range(0, len(parts), 2)]
    return parts[0]


def table_rounds(count):
    twos = []
    stride = 1
    while count % (2 * stride) == 0:
        twos.append(stride)
        stride *= 2
    order = ROUND_ORDER
    rounds = [tuple(twos[d] for d in digits if d < len(twos)) for digits in order]
    used = sum(len(digits) for digits in order)
    rounds += [(twos[d],) for d in range(used, len(twos))]
    odd = []
    rest, factor = count // stride, 3
    while rest > 1:
        while rest % factor == 0:
            odd.append((stride, factor))
            stride *= factor
            rest //= factor
        factor += 2
    return [r for r in rounds if r], odd


def all_sum(part):
    count = lax.axis_size(AXES)
    me = lax.axis_index(AXES)
    binary, odd = table_rounds(count)
    at = 0
    for strides in binary:
        masks = [0]
        for stride in strides:
            masks += [mask ^ stride for mask in masks]
        parts = [part]
        for mask in masks[1:]:
            parts.append(lax.ppermute(part, AXES, [(i, i ^ mask) for i in range(count)]))
        if at == len(binary) - 1 and not odd:
            return parts
        part = pair_tree(parts)
        at += 1
    for stride, radix in odd:
        digit = (me // stride) % radix
        parts = [part]
        for step in range(1, radix):
            route = []
            for i in range(count):
                d = (i // stride) % radix
                route.append((i, i + (((d - step) % radix) - d) * stride))
            parts.append(lax.ppermute(part, AXES, route))
        total = jnp.zeros_like(part)
        for d in range(radix):
            value = parts[0]
            for step in range(1, radix):
                value = jnp.where((digit + step) % radix == d, parts[step], value)
            total = total + value
        part = total
        at += 1
    return [part]


def prep_tiles(head_count, table_ref, chunk_ref, tile_ref):
    size = tile_ref.shape[2]
    table_len = table_ref.shape[1]
    span = chunk_ref.shape[1]
    pad = size - (SEG_LEN - 1)
    lane = lax.broadcasted_iota(jnp.int32, (head_count, span), 1)
    table = table_ref[...] * LOG2E
    first, last = table[:, :1], table[:, table_len - 1 :]
    wide = jnp.concatenate([table, jnp.zeros((head_count, span - table_len), F32)], axis=1)
    moved = pltpu.roll(wide, pad, 1)
    moved = jnp.where(lane < pad, first, jnp.where(lane >= pad + table_len, last, moved))
    chunk_ref[...] = moved
    row = lax.broadcasted_iota(jnp.int32, (size, size), 0)
    col = lax.broadcasted_iota(jnp.int32, (size, size), 1)

    @pl.loop(0, head_count)
    def _(head):
        rolled = []
        lines = chunk_ref[pl.ds(head, 1), :]
        for c in range(4):
            line = jnp.broadcast_to(lines[:, c * size : (c + 1) * size], (size, size))
            rolled.append(pltpu.roll(line, 0, 1, stride=1, stride_axis=0))
        for b in range(3):
            tile = jnp.where(col >= row, rolled[b + 1], rolled[b])
            if b == 0:
                tile = jnp.where((row // SEG_LEN) <= (col // SEG_LEN), tile, MASKED)
            tile_ref[head, b] = tile


def unroll_sum(tile):
    size = tile.shape[0]
    group = 8
    parts = []
    for start in range(0, size, group):
        part = tile[start : start + group, :]
        parts.append(part if start == 0 else pltpu.roll(part, size - start, 1))
    total = pair_tree(parts)
    row = lax.broadcasted_iota(jnp.int32, total.shape, 0)
    for bit in (1, 2, 4):
        total = jnp.where((row & bit) != 0, pltpu.roll(total, size - bit, 1), total)
    return jnp.sum(total, axis=0, keepdims=True)


def score_terms(lag, raw_ref, wgt_ref, w_ref, s_ref, log_row, dot_row, tiles, const, inv_root):
    half = raw_ref.shape[0] // 2
    row = lax.broadcasted_iota(jnp.int32, (half, half), 0) // SEG_LEN
    col = lax.broadcasted_iota(jnp.int32, (half, half), 1) // SEG_LEN
    acc = [None, None, None, None]
    for r in range(2):
        for c in range(2):
            rs, cs = slice(r * half, (r + 1) * half), slice(c * half, (c + 1) * half)
            if (lag == 0 and r > c) or (lag == 2 and c > r):
                w_ref[rs, cs] = jnp.zeros((half, half), BF16)
                s_ref[rs, cs] = jnp.zeros((half, half), BF16)
                continue
            level = min(2 * lag + c - r, 3)
            lrow = log_row[:, cs]
            bias = const - lrow if level == 3 else tiles[level] - lrow
            weight = jnp.exp2(raw_ref[rs, cs] * (inv_root * LOG2E) + bias)
            if lag == 2 and r == c:
                weight = jnp.where(col <= row, weight, 0.0)
            score = weight * (wgt_ref[rs, cs] - dot_row[:, cs])
            acc[level] = score if acc[level] is None else acc[level] + score
            w_ref[rs, cs] = weight.astype(BF16)
            s_ref[rs, cs] = score.astype(BF16)
    return acc


def table_lines(acc, size):
    row = lax.broadcasted_iota(jnp.int32, (size, size), 0)
    col = lax.broadcasted_iota(jnp.int32, (size, size), 1)
    zero = jnp.zeros((size, size), F32)
    lines = []
    for c in range(4):
        upper = acc[c - 1] if c > 0 else None
        lower = acc[c] if c < 3 else None
        line = None
        if upper is not None or lower is not None:
            mixed = jnp.where(
                col >= row,
                zero if upper is None else upper,
                zero if lower is None else lower,
            )
            line = unroll_sum(mixed)
        if c == 3 and acc[3] is not None:
            extra = jnp.sum(acc[3], axis=0, keepdims=True)
            line = extra if line is None else line + extra
        lines.append(line)
    return lines


def fold_table(lines, table_len, size):
    pad = size - (SEG_LEN - 1)
    lane = lax.broadcasted_iota(jnp.int32, lines.shape, 1)
    tail = jnp.sum(jnp.where(lane >= pad + table_len - 1, lines, 0.0), axis=1, keepdims=True)
    moved = pltpu.roll(lines, lines.shape[1] - pad, 1)[:, :table_len]
    lane = lax.broadcasted_iota(jnp.int32, moved.shape, 1)
    return jnp.where(lane == table_len - 1, tail, moved)


def pack_height(count, rows, width):
    lines = -(-count * TERMS * rows // width)
    return -(-lines // 8) * 8


def pack_lines(stats, width):
    count, rows = stats.shape
    high = stats.astype(BF16).astype(F32)
    rest = stats - high
    mid = rest.astype(BF16).astype(F32)
    terms = (high, mid, rest - mid)
    per_row = width // rows
    lines = []
    for line in range(pack_height(count, rows, width)):
        pieces = []
        for b in range(line * per_row, (line + 1) * per_row):
            if b < count * TERMS:
                pieces.append(terms[b // count][b % count : b % count + 1, :])
            else:
                pieces.append(jnp.zeros((1, rows), F32))
        lines.append(jnp.concatenate(pieces, axis=1))
    return jnp.concatenate(lines, axis=0).astype(BF16)


def unpack_lines(pack_ref, stat_ref):
    count, rows = stat_ref.shape
    per_row = pack_ref.shape[1] // rows
    packed = pack_ref[rows:, :].astype(F32)
    for i in range(count):
        total = None
        for term in range(TERMS):
            line, at = divmod(term * count + i, per_row)
            piece = packed[line : line + 1, at * rows : (at + 1) * rows]
            total = piece if total is None else total + piece
        stat_ref[i : i + 1, :] = total


def prep_kernel(g_hbm, log_hbm, dot_hbm, far_ref, first_ref, second_ref, stat_ref,
                log_ref, dot_ref, sems):
    rows, feats = g_hbm.shape
    cut = first_ref.shape[1]
    moves = (
        (log_hbm, log_ref),
        (dot_hbm, dot_ref),
        (g_hbm, far_ref.at[pl.ds(0, rows), :]),
        (g_hbm.at[:, pl.ds(0, cut)], first_ref.at[pl.ds(0, rows), :]),
        (g_hbm.at[:, pl.ds(cut, feats - cut)], second_ref),
    )
    copies = []
    for i, (origin, target) in enumerate(moves):
        copies.append(pltpu.make_async_copy(origin, target, sems.at[i]))
        copies[-1].start()
    for copy in copies[:2]:
        copy.wait()
    stats = jnp.concatenate([log_ref[...] * LOG2E, dot_ref[...]], axis=0)
    stat_ref[...] = stats
    first_ref[rows:, :] = pack_lines(stats, first_ref.shape[1])
    far_ref[rows:, :] = pack_lines(stats, far_ref.shape[1])
    for copy in copies[2:]:
        copy.wait()


def lag_kernel(lag, first_head, last_head, head_count, *refs):
    raw_refs, wgt_refs, w_refs, s_refs = (refs[len(refs) - 8 + 2 * i :][:2] for i in range(4))
    refs = refs[:-8]
    if lag == 0:
        (k_hbm, v_hbm, q_hbm, table_hbm, g_ref, stat_ref,
         dq_ref, dk_ref, dv_ref, tab_ref, kt_ref, tile_ref, chunk_ref, k_ref, v_ref,
         q_ref, table_ref, sems) = refs
        pairs = ((table_hbm, table_ref), (k_hbm, k_ref), (v_hbm, v_ref), (q_hbm, q_ref))
        copies = []
        for i, (source, target) in enumerate(pairs):
            copies.append(pltpu.make_async_copy(source, target, sems.at[i]))
            copies[-1].start()
        copies[0].wait()
        prep_tiles(head_count, table_ref, chunk_ref, tile_ref)
        for copy in copies[1:]:
            copy.wait()
    elif lag == 2:
        (k_ref, v_ref, kt_ref, tile_ref, chunk_ref, dk_in, dv_in, tab_in, q_ref, g_ref,
         dk_ref, dv_ref, tab_ref, dq_ref, stat_ref) = refs
        unpack_lines(g_ref, stat_ref)
    elif first_head == 0:
        (k_ref, v_ref, kt_ref, tile_ref, chunk_ref, dk_in, dv_in, tab_in, q_ref, g_ref,
         dk_ref, dv_ref, tab_ref, dq_ref, stat_ref) = refs
        unpack_lines(g_ref, stat_ref)
    else:
        (k_ref, v_ref, kt_ref, tile_ref, chunk_ref, dk_in, dv_in, tab_in, q_ref, g_ref,
         stat_ref, _, dk_ref, dv_ref, out_tab_ref, dq_ref) = refs
    rows = k_ref.shape[0]
    size = tile_ref.shape[2]
    head_dim = k_ref.shape[1] // head_count
    inv_root = head_dim ** (-0.5)
    g_shift = -first_head * head_dim
    last_lines = []

    def span(head):
        return slice(head * head_dim, (head + 1) * head_dim)

    def products(head, at):
        local = slice(head * head_dim + g_shift, (head + 1) * head_dim + g_shift)
        query, grad = q_ref[:, span(head)], g_ref[:rows, local]
        raw_refs[at][...] = lax.dot_general(
            k_ref[:, span(head)], query, NT, preferred_element_type=F32
        )
        wgt_refs[at][...] = lax.dot_general(
            v_ref[:, span(head)], grad, NT, preferred_element_type=F32
        )

    def scores(head, at):
        log_row = stat_ref[head : head + 1, :]
        dot_row = stat_ref[head + head_count : head + head_count + 1, :]
        const = chunk_ref[head : head + 1, 3 * size :]
        tiles = [None if lag == 2 else tile_ref[head, b] for b in range(3)]
        acc = score_terms(
            lag, raw_refs[at], wgt_refs[at], w_refs[at], s_refs[at],
            log_row, dot_row, tiles, const, inv_root,
        )
        lines = [
            jnp.zeros((1, size), F32) if line is None else line for line in table_lines(acc, size)
        ]
        lines = jnp.concatenate(lines, axis=1)
        if lag > 0:
            lines = tab_in[head : head + 1, :] + lines
        if first_head == 0:
            tab_ref[head : head + 1, :] = lines
        else:
            last_lines.append(lines)

    def gradients(head, at):
        cols = span(head)
        local = slice(head * head_dim + g_shift, (head + 1) * head_dim + g_shift)
        if lag == 0:
            turned = k_ref[:, cols].T
            kt_ref[cols, :] = turned
        else:
            turned = kt_ref[cols, :]
        score_b = s_refs[at][...]
        dq = lax.dot_general(turned, score_b, NN, preferred_element_type=F32) * inv_root
        dq_ref[cols, :] = dq.astype(dq_ref.dtype)
        dk = lax.dot_general(score_b, q_ref[:, cols], NN, preferred_element_type=F32)
        dv = lax.dot_general(w_refs[at][...], g_ref[:rows, local], NN, preferred_element_type=F32)
        if lag > 0:
            dk = dk + dk_in[:, cols]
            dv = dv + dv_in[:, cols]
        dk_ref[:, cols] = dk
        dv_ref[:, cols] = dv

    stages = (products, scores, gradients)
    steps = last_head - first_head + len(stages) - 1
    for step in range(steps):
        for depth, stage in enumerate(stages):
            head = first_head + step - depth
            if first_head <= head < last_head:
                stage(head, head % 2)

    if first_head > 0:
        table = jnp.concatenate([tab_in[:first_head, :]] + last_lines, axis=0)
        out_tab_ref[...] = fold_table(table, out_tab_ref.shape[1], size)


def key_value_kernel(scale, dk_ref, dv_ref, gk_hbm, gv_hbm, gk_ref, gv_ref, sems):
    gk_ref[...] = (dk_ref[...] * scale).astype(BF16)
    copies = [pltpu.make_async_copy(gk_ref, gk_hbm, sems.at[0])]
    copies[0].start()
    gv_ref[...] = dv_ref[...].astype(BF16)
    copies.append(pltpu.make_async_copy(gv_ref, gv_hbm, sems.at[1]))
    copies[1].start()
    for copy in copies:
        copy.wait()


def query_kernel(head_count, dq_ref, one_ref, two_ref, *refs):
    term_refs = refs[:-5]
    gq_hbm, table_hbm, gq_ref, table_ref, sems = refs[-5:]
    table_ref[...] = pair_tree([ref[...] for ref in term_refs])
    head_dim = dq_ref.shape[0] // head_count
    copies = [pltpu.make_async_copy(table_ref, table_hbm, sems.at[0])]
    copies[0].start()
    for head in range(head_count):
        cols = slice(head * head_dim, (head + 1) * head_dim)
        total = dq_ref[cols, :] + one_ref[cols, :].astype(F32) + two_ref[cols, :].astype(F32)
        gq_ref[:, cols] = total.astype(BF16).T
        if head % 2 == 1:
            part = pl.ds((head - 1) * head_dim, 2 * head_dim)
            copies.append(
                pltpu.make_async_copy(gq_ref.at[:, part], gq_hbm.at[:, part], sems.at[1 + head // 2])
            )
            copies[-1].start()
    for copy in copies:
        copy.wait()


def local(query_rows, key_rows, value_rows, out_grad, log_totals, out_dot, bias_table):
    rows, feats = query_rows.shape
    heads = log_totals.shape[1]
    table_len = bias_table.shape[1]
    half = rows // 2
    cut_head = heads * 3 // 4
    head_dim = feats // heads
    cut = cut_head * head_dim
    vmem = pl.BlockSpec(memory_space=pltpu.VMEM)
    hbm = pl.BlockSpec(memory_space=pltpu.HBM)
    pair_flops = 2 * rows * rows * head_dim

    def call(body, work, outs, args, scratch=(), specs=None, out_specs=None, aliases={}):
        estimate = pl.CostEstimate(
            flops=int(work * pair_flops), bytes_accessed=8 * rows * feats, transcendentals=0
        )
        return pl.pallas_call(
            body,
            in_specs=[vmem] * len(args) if specs is None else specs,
            out_specs=[vmem] * len(outs) if out_specs is None else out_specs,
            out_shape=outs,
            scratch_shapes=list(scratch),
            input_output_aliases=aliases,
            cost_estimate=estimate,
            compiler_params=pltpu.CompilerParams(vmem_limit_bytes=16 * 2**20),
        )(*args)

    rows_f32 = pltpu.VMEM((rows, feats), F32)
    rows_b16 = pltpu.VMEM((rows, feats), BF16)
    turn_f32 = pltpu.VMEM((feats, rows), F32)
    turn_b16 = pltpu.VMEM((feats, rows), BF16)
    wide_tab = pltpu.VMEM((heads, 4 * half), F32)
    table_shape = pltpu.VMEM((heads, table_len), F32)
    tile_shape = pltpu.VMEM((heads, 3, half, half), F32)
    stat_shape = pltpu.VMEM((2 * heads, rows), F32)
    line_shape = pltpu.VMEM((heads, rows), F32)
    out_shape = jax.ShapeDtypeStruct((rows, feats), BF16)
    stage_shapes = (pltpu.VMEM((rows, rows), F32),) * 4 + (pltpu.VMEM((rows, rows), BF16),) * 4
    body = functools.partial

    def at_hbm(array):
        return pltpu.with_memory_space_constraint(array, pltpu.HBM)

    def packed_shape(height, width):
        return pltpu.VMEM((height + pack_height(2 * heads, rows, width), width), BF16)

    query_far = shifted(query_rows, -2)
    query_in = shifted(query_rows, -1)
    far, first, second, stats = call(
        prep_kernel, 1,
        [packed_shape(rows, feats), packed_shape(rows, cut),
         pltpu.VMEM((rows, feats - cut), BF16), stat_shape],
        tuple(at_hbm(x) for x in (out_grad, log_totals.T, out_dot.T)),
        (line_shape, line_shape, pltpu.SemaphoreType.DMA((5,))),
        [hbm] * 3,
    )
    far_in = shifted(far, -2)
    first_in = shifted(first, -1)
    second_in = shifted(second, -1)

    dq0, dk, dv, tab, turned, tiles, chunks, keys, values = call(
        body(lag_kernel, 0, 0, heads, heads), 5 * heads,
        [turn_f32, rows_f32, rows_f32, wide_tab, turn_b16, tile_shape, wide_tab,
         rows_b16, rows_b16],
        tuple(at_hbm(x) for x in (key_rows, value_rows, query_rows, bias_table))
        + (far, stats),
        (rows_b16, table_shape, pltpu.SemaphoreType.DMA((4,))) + stage_shapes,
        [hbm] * 4 + [vmem] * 2,
    )
    shared = (keys, values, turned, tiles, chunks)
    dk, dv, tab, dq2, _ = call(
        body(lag_kernel, 2, 0, heads, heads), 5 * heads,
        [rows_f32, rows_f32, wide_tab, turn_b16, stat_shape],
        shared + (dk, dv, tab, query_far, far_in), stage_shapes, aliases={5: 0, 6: 1, 7: 2},
    )
    back_far = shifted(dq2, 2)
    dk, dv, tab, dq1, stats_in = call(
        body(lag_kernel, 1, 0, cut_head, heads), 5 * cut_head,
        [rows_f32, rows_f32, wide_tab, turn_b16, stat_shape],
        shared + (dk, dv, tab) + (query_in, first_in), stage_shapes, aliases={5: 0, 6: 1, 7: 2},
    )
    dk, dv, table_part, dq1 = call(
        body(lag_kernel, 1, cut_head, heads, heads), 5 * (heads - cut_head),
        [rows_f32, rows_f32, table_shape, turn_b16],
        shared + (dk, dv, tab) + (query_in, second_in, stats_in, dq1), stage_shapes,
        aliases={5: 0, 6: 1, 11: 3},
    )
    back_near = shifted(dq1, 1)
    table_terms = all_sum(table_part)
    grad_key, grad_value = call(
        body(key_value_kernel, head_dim ** (-0.5)), 1, [out_shape] * 2, (dk, dv),
        (rows_b16,) * 2 + (pltpu.SemaphoreType.DMA((2,)),), out_specs=[hbm] * 2,
    )
    table_out = jax.ShapeDtypeStruct((heads, table_len), F32)
    grad_query, grad_table = call(
        body(query_kernel, heads), 1, [out_shape, table_out],
        (dq0, back_near, back_far, *table_terms),
        (rows_b16, table_shape, pltpu.SemaphoreType.DMA((1 + heads // 2,))),
        out_specs=[hbm] * 2,
    )
    return grad_query, grad_key, grad_value, grad_table


def solution(mesh):
    placed = (P(AXES, None),) * 6 + (P(),)
    return jax.shard_map(
        local,
        mesh=mesh,
        in_specs=placed,
        out_specs=(P(AXES, None),) * 3 + (P(),),
        check_vma=False,
    )
```
